32 devices in a mesh: sp: 8 (over z, x), tp: 4 (over y, core).
Axes of the slice: x: 2, y: 2, z: 4, core: 2. Of those that a mesh axis runs over, the one named last changes fastest.
Arguments:
- residual: bfloat16 [4096, 4096], P('sp'), may hold values from -6 to 6
- queries: bfloat16 [4096, 1024], P('sp', 'tp'), may hold values from -6 to 6
- projected_key_rows: bfloat16 [4096, 1024], P('sp', 'tp'), may hold values from -6 to 6
- projected_value_rows: bfloat16 [4096, 2048], P('sp', 'tp'), may hold values from -6 to 6
- output_gate_logits: bfloat16 [4096, 2048], P('sp', 'tp'), may hold values from -6 to 6
- input_gate_logits: float32 [16, 4096], P('tp', 'sp'), may hold values from -8 to 120
- forget_gate_logits: float32 [16, 4096], P('tp', 'sp'), may hold values from 0 to 16
- extra_forget_logits: float32 [16, 4096], P('tp', 'sp'), may hold values from -0.7 to 0, as said below
- head_norm_gain: bfloat16 [2048], P('tp'), may hold values from 0.099609375 to 1.8984375
- output_projection_weight: bfloat16 [2048, 4096], P('tp'), may hold values from -0.125 to 0.125
- feedforward_norm_gain: bfloat16 [4096], replicated, may hold values from 0.099609375 to 1.8984375
- feedforward_gate_weight: bfloat16 [4096, 11264], P('sp', 'tp'), may hold values from -0.09375 to 0.09375
- up_projection_weight: bfloat16 [4096, 11264], P('sp', 'tp'), may hold values from -0.09375 to 0.09375
- down_projection_weight: bfloat16 [4096, 11264], P('sp', 'tp'), may hold values from -0.0546875 to 0.0546875
Outputs:
- layer_out: bfloat16 [4096, 4096], P(('sp', 'tp'))
The draws below stay inside these ranges and needn't reach their ends.
Inputs may be any that keep to these rules, and one draw needn't show every extreme that they name: `extra_forget_logits`: each entry is 0 or the logarithm of a factor between one half and 0.8.
All inputs are finite; a program needn't handle non-finite values.
Results may differ from the reference program's by a relative error of at most 0.01.
Values may be sent and summed in bfloat16 or wider, within the bound.
A program may use at most 192 MiB of HBM per device.

```python
import math
import jax
import jax.numpy as jnp
from jax import lax

D = 4096
HEADS = 16
QK_DIM = 64
V_DIM = 128
FF = 11264
BLOCK = 64
TOK_DEV = 512
TOKENS = 4096
VW = 2048
N_TP = 4


def draw_input_gate_logits(key, part):
    values = jnp.clip(1.5 * jax.random.normal(jax.random.fold_in(key, 11), (HEADS, TOKENS), jnp.float32), -6.0, 6.0)
    return values.astype(jnp.float32)


def draw_forget_gate_logits(key, part):
    slow = jax.random.bernoulli(jax.random.fold_in(key, 21), 0.5, (HEADS, 1))
    noise = 0.7 * jax.random.normal(jax.random.fold_in(key, 22), (HEADS, TOKENS), jnp.float32)
    base = jnp.where(slow, math.log(TOKENS) + 1.5, 3.5)
    shift = jax.random.uniform(jax.random.fold_in(key, 23), (HEADS, TOKENS // TOK_DEV), jnp.float32, -0.7, 0.7)
    values = base + noise + jnp.repeat(shift, TOK_DEV, axis=1)
    return jnp.clip(values, 0.0, 16.0).astype(jnp.float32)


def draw_extra_forget_logits(key, part):
    hits = jax.random.bernoulli(jax.random.fold_in(key, 31), 4.0 / TOKENS, (HEADS, TOKENS))
    factor = jax.random.uniform(jax.random.fold_in(key, 32), (HEADS, TOKENS), jnp.float32, 0.5, 0.8)
    return jnp.where(hits, jnp.log(factor), 0.0).astype(jnp.float32)


def block_levels(rng, shape, split, least, top_value):
    def one(dim, parts):
        draws = jax.random.uniform(jax.random.fold_in(jax.random.fold_in(rng, 6), dim), (parts,), jnp.float32, least / len(split), top_value / len(split))
        return jnp.repeat(jnp.exp(draws), shape[dim] // parts).reshape((-1,) + (1,) * (len(shape) - dim - 1))

    level = one(*split[0])
    for cut in split[1:]:
        level = level * one(*cut)
    return level


def centred(key, extent, scale, bound, cuts=(), kind=jnp.bfloat16):
    drawn = scale * jax.random.normal(key, extent, jnp.float32)
    if cuts:
        drawn = drawn * block_levels(key, extent, cuts, -0.22, 0.18)
    return jnp.clip(drawn, -bound, bound).astype(kind)


def setup_inputs(seed: int = 0) -> dict:
    streams_of = jax.random.split(jax.random.key(seed), 15)
    residual = centred(streams_of[0], (TOKENS, D), 1.0, 6.0, ((0, 8),))
    queries = centred(streams_of[1], (TOKENS, HEADS * QK_DIM), 1.0, 6.0, ((0, 8), (1, 4)))
    projected_key_rows = centred(streams_of[2], (TOKENS, HEADS * QK_DIM), 1.0, 6.0, ((0, 8), (1, 4)))
    projected_value_rows = centred(streams_of[3], (TOKENS, VW), 1.0, 6.0, ((0, 8), (1, 4)))
    output_gate_logits = centred(streams_of[4], (TOKENS, VW), 1.0, 6.0, ((0, 8), (1, 4)))
    input_gate_logits = draw_input_gate_logits(jax.random.fold_in(streams_of[14], 71), 0)
    forget_gate_logits = draw_forget_gate_logits(jax.random.fold_in(streams_of[14], 71), 0)
    extra_forget_logits = draw_extra_forget_logits(jax.random.fold_in(streams_of[14], 71), 0)
    head_norm_gain = jnp.clip(1.0 + 0.18 * jax.random.normal(streams_of[8], (VW,), jnp.float32), 0.099609375, 1.8984375).astype(jnp.bfloat16)
    output_projection_weight = centred(streams_of[9], (VW, D), VW ** -0.5, 0.125, ((0, 4),))
    feedforward_norm_gain = jnp.clip(1.0 + 0.18 * jax.random.normal(streams_of[10], (D,), jnp.float32), 0.099609375, 1.8984375).astype(jnp.bfloat16)
    feedforward_gate_weight = centred(streams_of[11], (D, FF), D ** -0.5, 0.09375, ((0, 8), (1, 4)))
    up_projection_weight = centred(streams_of[12], (D, FF), D ** -0.5, 0.09375, ((0, 8), (1, 4)))
    down_projection_weight = centred(streams_of[13], (D, FF), FF ** -0.5, 0.0546875, ((0, 8), (1, 4)))
    return {"residual": residual, "queries": queries, "projected_key_rows": projected_key_rows, "projected_value_rows": projected_value_rows, "output_gate_logits": output_gate_logits, "input_gate_logits": input_gate_logits, "forget_gate_logits": forget_gate_logits, "extra_forget_logits": extra_forget_logits, "head_norm_gain": head_norm_gain, "output_projection_weight": output_projection_weight, "feedforward_norm_gain": feedforward_norm_gain, "feedforward_gate_weight": feedforward_gate_weight, "up_projection_weight": up_projection_weight, "down_projection_weight": down_projection_weight}


def run_blocks(query_h, key_h, value_h, gate_in, forget_logarithm, state_init, norm_init, peak_init):
    span_len = BLOCK
    blocks_count = query_h.shape[0] // span_len
    query_b = query_h.reshape(blocks_count, span_len, query_h.shape[1])
    key_b = key_h.reshape(blocks_count, span_len, key_h.shape[1])
    value_b = value_h.reshape(blocks_count, span_len, value_h.shape[1])
    gate_b = gate_in.reshape(blocks_count, span_len)
    cum_local = jnp.cumsum(forget_logarithm.reshape(blocks_count, span_len), axis=1)
    cum_last = cum_local[:, -1]
    log_end = cum_last[:, None] - cum_local + gate_b

    def advance(carry, inputs):
        state_now, norm_now, peak_now = carry
        key_blk, value_blk, log_blk, last_blk = inputs
        peak_next = jnp.maximum(last_blk + peak_now, jnp.max(log_blk))
        decay_now = jnp.exp(last_blk + peak_now - peak_next)
        weights = jnp.exp(log_blk - peak_next)
        state_next = decay_now * state_now + jnp.einsum('l,lv,lk->vk', weights, value_blk, key_blk, precision=lax.Precision.HIGHEST)
        norm_next = decay_now * norm_now + jnp.einsum('l,lk->k', weights, key_blk, precision=lax.Precision.HIGHEST)
        return ((state_next, norm_next, peak_next), (state_now, norm_now, peak_now))
    carried, (state_prev, norm_prev, peak_prev) = lax.scan(advance, (state_init, norm_init, peak_init), (key_b, value_b, log_end, cum_last))
    causal = jnp.tril(jnp.ones((span_len, span_len), dtype=bool))
    log_pair = cum_local[:, :, None] - cum_local[:, None, :] + gate_b[:, None, :]
    log_pair = jnp.where(causal[None], log_pair, -jnp.inf)
    inter_log = cum_local + peak_prev[:, None]
    peak_row = jnp.maximum(inter_log, lax.optimization_barrier(jnp.max(log_pair, axis=2)))
    scores = jnp.einsum('cjk,csk->cjs', query_b, key_b, precision=lax.Precision.HIGHEST) * jnp.exp(log_pair - peak_row[:, :, None])
    inter_scale = jnp.exp(inter_log - peak_row)
    numer = jnp.einsum('cjs,csv->cjv', scores, value_b, precision=lax.Precision.HIGHEST)
    numer = numer + inter_scale[:, :, None] * jnp.einsum('cjk,cvk->cjv', query_b, state_prev, precision=lax.Precision.HIGHEST)
    denominator = lax.optimization_barrier(jnp.sum(scores, axis=2)) + inter_scale * jnp.einsum('cjk,ck->cj', query_b, norm_prev, precision=lax.Precision.HIGHEST)
    cell_out = numer / jnp.maximum(jnp.abs(denominator), jnp.exp(-peak_row))[:, :, None]
    return cell_out.reshape(query_h.shape[0], value_h.shape[1])

def by_heads(rows, heads_count):
    tok_count = rows.shape[0]
    return rows.astype(jnp.float32).reshape(tok_count, heads_count, rows.shape[1] // heads_count).transpose(1, 0, 2)

def rms_scaled(values_f32, gain):
    mean_square = lax.optimization_barrier(jnp.mean(values_f32 * values_f32, axis=-1, keepdims=True))
    return values_f32 * lax.rsqrt(mean_square + 1e-06) * gain.astype(jnp.float32)

def reference(residual, queries, projected_key_rows, projected_value_rows, output_gate_logits, input_gate_logits, forget_gate_logits, extra_forget_logits, head_norm_gain, output_projection_weight, feedforward_norm_gain, feedforward_gate_weight, up_projection_weight, down_projection_weight):
    query_h = by_heads(queries, HEADS) * QK_DIM ** (-0.5)
    key_h = by_heads(projected_key_rows, HEADS)
    value_h = by_heads(projected_value_rows, HEADS)
    forget_logarithm = jax.nn.log_sigmoid(forget_gate_logits) + extra_forget_logits
    state_zero = jnp.zeros((HEADS, V_DIM, QK_DIM), jnp.float32)
    norm_zero = jnp.zeros((HEADS, QK_DIM), jnp.float32)
    peak_zero = jnp.zeros((HEADS,), jnp.float32)
    cell_out = jax.vmap(run_blocks)(query_h, key_h, value_h, input_gate_logits, forget_logarithm, state_zero, norm_zero, peak_zero)
    normed_heads = rms_scaled(cell_out, head_norm_gain.reshape(HEADS, 1, V_DIM))
    gated = (normed_heads.transpose(1, 0, 2).reshape(TOKENS, VW) * jax.nn.sigmoid(output_gate_logits.astype(jnp.float32))).astype(jnp.bfloat16)
    group_cols = VW // N_TP
    attn_sum = jnp.zeros((TOKENS, D), jnp.float32)
    for group in range(N_TP):
        partial_out = jnp.dot(gated[:, group * group_cols:(group + 1) * group_cols], output_projection_weight[group * group_cols:(group + 1) * group_cols], preferred_element_type=jnp.float32).astype(jnp.bfloat16)
        attn_sum = attn_sum + lax.optimization_barrier(partial_out).astype(jnp.float32)
    stream = residual.astype(jnp.float32) + attn_sum
    normed = rms_scaled(stream, feedforward_norm_gain).astype(jnp.bfloat16)
    gate_pre = jnp.dot(normed, feedforward_gate_weight, preferred_element_type=jnp.float32)
    up_pre = jnp.dot(normed, up_projection_weight, preferred_element_type=jnp.float32)
    hidden = (jax.nn.silu(gate_pre) * up_pre).astype(jnp.bfloat16)
    hidden_cols = FF // N_TP
    ffn_sum = jnp.zeros((TOKENS, D), jnp.float32)
    for group in range(N_TP):
        partial_ffn = lax.dot_general(hidden[:, group * hidden_cols:(group + 1) * hidden_cols], down_projection_weight[:, group * hidden_cols:(group + 1) * hidden_cols], (((1,), (1,)), ((), ())), preferred_element_type=jnp.float32).astype(jnp.bfloat16)
        ffn_sum = ffn_sum + lax.optimization_barrier(partial_ffn).astype(jnp.float32)
    return (stream + 0.5 * ffn_sum).astype(jnp.bfloat16)
```

```python
import functools
import jax
import jax.numpy as jnp
from jax import lax
from jax.experimental import pallas as pl
from jax.experimental.pallas import tpu as pltpu
from jax.sharding import PartitionSpec as P

MESH = pl.DeviceIdType.MESH
F32 = jnp.float32
BF16 = jnp.bfloat16
LANES = 128
QUERY_ROWS = 256
TOKEN_ROWS = 256
GATHER_CUTS = 2
EARLY_GROUPS = 3


class Plan:
    def __init__(self, mesh_shape, shapes):
        self.sp, self.tp = mesh_shape["sp"], mesh_shape["tp"]
        self.nz = next(n for n in range(1, self.sp + 1) if self.sp % n == 0 and n * n >= self.sp)
        self.nx = self.sp // self.nz
        self.nc = 2
        self.ny = self.tp // self.nc
        self.tok, self.d = shapes["residual"]
        self.own = self.tok // self.tp
        self.heads = shapes["gates"][0]
        self.qk = shapes["queries"][1] // self.heads
        self.vd = shapes["values"][1] // self.heads
        self.per = LANES // self.qk
        self.pairs = self.heads // self.per
        self.vw = shapes["values"][1]
        self.rows, self.ff = shapes["gate"]
        self.zc = self.nz // self.nc
        tiles = self.ff // LANES
        wide = -(-tiles // self.zc)
        starts = [min(i * wide, tiles - wide) for i in range(self.zc)]
        self.start = [s * LANES for s in starts]
        self.dup = [(i * wide - s) * LANES for i, s in enumerate(starts)]
        self.hid = wide * LANES
        self.nj = self.rows // LANES
        self.halves = 2
        self.sph = self.sp // self.halves
        self.cw = self.sph * LANES
        self.ns = self.nj * self.halves
        self.toks = self.nz * self.ny * self.own
        self.state_rows = self.pairs * LANES + -(-(self.pairs + 2 * self.heads) // 8) * 8
        self.wc = next(
            n for n in range(self.hid // LANES * LANES, 0, -LANES) if self.d % n == 0
        )
        self.cc = min(self.cw, self.wc)


def dotf(a, b, dims=(((1,), (0,)), ((), ())), precision=None):
    return lax.dot_general(a, b, dims, preferred_element_type=F32, precision=precision)


def split(a):
    high = a.astype(BF16)
    return high, (a - high.astype(F32)).astype(BF16)


def layer(p, *refs):
    (
        residual, queries, keys, values, out_gate, in_gate, forget, extra, head_gain, out_w,
        ff_gain, gate_w, up_w, down_w,
        out, gate_b, up_b, down_b,
        col, gated, xs, zs, carry, tokens, acc, slab, parts, yb, lb, rb, stream, cr, yr, res,
        s1_send, s1_recv, xf_send, xf_recv, pf_send, pf_recv,
        stx_send, stx_recv, stz_send, stz_recv, at_send, at_recv, ay_send, ay_recv,
        gz_right, gz_left, gz_recv, gy_send, gy_recv,
        ry_send, ry_recv, rr_send, rl_send, rl_recv, rr_recv, local,
    ) = refs
    nz, nx, ny, nc = p.nz, p.nx, p.ny, p.nc
    sp_i, tp_i = lax.axis_index("sp"), lax.axis_index("tp")
    z, x = sp_i // nx, lax.rem(sp_i, nx)
    y, c = tp_i // nc, lax.rem(tp_i, nc)
    other = 1 - c
    duty = c == 1 - z // p.zc

    def dev(z_, x_, y_, c_):
        return (z_ * nx + x_, y_ * nc + c_)

    def mod(a, e, n):
        return lax.rem(a + e, n)

    def remote(src, dst, send, recv, device):
        return pltpu.make_async_remote_copy(
            src_ref=src, dst_ref=dst, send_sem=send, recv_sem=recv,
            device_id=device, device_id_type=MESH,
        )

    barrier = pltpu.get_barrier_semaphore()
    friends = [dev(mod(z, e, nz), x, y, c) for e in range(1, nz)]
    friends += [dev(z, mod(x, e, nx), y, c) for e in range(1, nx)]
    friends += [dev(z, x, mod(y, e, ny), c) for e in range(1, ny)]
    friends += [dev(mod(z, e, nz), x, y, other) for e in range(nz)]
    for friend in friends:
        pl.semaphore_signal(barrier, inc=1, device_id=friend, device_id_type=MESH)
    pl.semaphore_wait(barrier, len(friends))

    mats = ((gate_w, gate_b), (up_w, up_b), (down_w, down_b))

    def jrows(j):
        return pl.ds(pl.multiple_of(j * LANES, LANES), LANES)

    def first_hop(m, j, i):
        src, dst = mats[m]
        return remote(
            src.at[jrows(j), pl.ds(p.start[i], p.hid)],
            dst.at[sp_i, jrows(j), :],
            s1_send.at[m, j, i], s1_recv.at[m, j, z],
            dev(c * p.zc + i, x, y, other),
        )

    def first_recv(m, j, zs_):
        src, dst = mats[m]
        view = dst.at[zs_ * nx + x, jrows(j), :]
        return remote(view, view, s1_send.at[m, j, 0], s1_recv.at[m, j, zs_], dev(z, x, y, other))

    def across(m, j, zs_, e):
        view = mats[m][1].at[zs_ * nx + x, jrows(j), :]
        return remote(
            view, view, xf_send.at[m, j, zs_, e - 1], xf_recv.at[m, j, zs_, e - 1],
            dev(z, mod(x, e, nx), y, c),
        )

    def across_recv(m, j, zs_, e):
        view = mats[m][1].at[zs_ * nx + mod(x, nx - e, nx), jrows(j), :]
        return remote(
            view, view, xf_send.at[m, j, zs_, e - 1], xf_recv.at[m, j, zs_, e - 1],
            dev(z, mod(x, e, nx), y, c),
        )

    def to_peer(m, j, sp_):
        view = mats[m][1].at[sp_, jrows(j), :]
        return remote(view, view, pf_send.at[m, j], pf_recv.at[m, j], dev(z, x, y, other))

    def peer_all(m, j):
        view = mats[m][1].at[:, jrows(j), :]
        return remote(view, view, pf_send.at[m, j], pf_recv.at[m, j], dev(z, x, y, other))

    def send_group(ms, j):
        for i in range(p.zc):
            for m in ms:
                first_hop(m, j, i).start()

    def each_z(fn):
        fn(z)
        for dist in range(1, nz):
            pl.when(z - dist >= 0)(functools.partial(fn, z - dist))
            pl.when(z + dist < nz)(functools.partial(fn, z + dist))

    def relay(ms, j):
        @pl.when(duty)
        def _():
            def one(zs_):
                for m in ms:
                    first_recv(m, j, zs_).wait_recv()
                    for e in range(1, nx):
                        across(m, j, zs_, e).start()
                    to_peer(m, j, zs_ * nx + x).start()

            each_z(one)

    def settle(ms, j):
        @pl.when(duty)
        def _():
            def one(zs_):
                for m in ms:
                    for e in range(1, nx):
                        across_recv(m, j, zs_, e).wait_recv()
                        to_peer(m, j, zs_ * nx + mod(x, nx - e, nx)).start()

            each_z(one)

        @pl.when(jnp.logical_not(duty))
        def _():
            for m in ms:
                peer_all(m, j).wait_recv()

    send_group((0, 1), 0)
    fetch_res = pltpu.make_async_copy(
        residual.at[pl.ds(pl.multiple_of(tp_i * p.own, p.own), p.own), :], res, local.at[2]
    )
    fetch_res.start()

    heads, per, pairs, tok = p.heads, p.per, p.pairs, p.tok
    fg = forget[...]
    lf = jnp.minimum(fg, 0.0) - jnp.log1p(jnp.exp(-jnp.abs(fg))) + extra[...]
    upper = (
        lax.broadcasted_iota(jnp.int32, (tok, tok), 0)
        <= lax.broadcasted_iota(jnp.int32, (tok, tok), 1)
    ).astype(F32)
    pad = jnp.zeros((-heads % 8, tok), F32)
    lf8 = jnp.concatenate([lf, pad], axis=0) if pad.shape[0] else lf
    cum_row = dotf(lf8, upper, precision=lax.Precision.HIGHEST)[:heads]
    ig = in_gate[...]
    pad = jnp.zeros((-2 * heads % 8, tok), F32)
    both = [cum_row, ig] + ([pad] if pad.shape[0] else [])
    col[...] = jnp.concatenate(both, axis=0).T
    bias_row = ig - cum_row
    base = pairs * LANES
    lane = lax.broadcasted_iota(jnp.int32, (1, LANES), 1) // p.qk
    subl = lax.broadcasted_iota(jnp.int32, (LANES, 1), 0) // p.qk

    def head_lanes(ref, h):
        pair = ref[:, h // per * LANES : (h // per + 1) * LANES]
        return jnp.where(lane == h % per, pair, jnp.zeros_like(pair))

    for pr in range(pairs):
        state = jnp.zeros((LANES, LANES), F32)
        norm = jnp.zeros((1, LANES), F32)
        for h in range(pr * per, (pr + 1) * per):
            total = cum_row[h : h + 1, tok - 1 : tok]
            log_w = total - col[:, h : h + 1] + col[:, heads + h : heads + h + 1]
            peak = jnp.max(log_w, axis=0, keepdims=True)
            weight = jnp.exp(log_w - peak)
            k_h = head_lanes(keys, h)
            high, low = split(values[:, h * p.vd : (h + 1) * p.vd].astype(F32) * weight)
            over = (((0,), (0,)), ((), ()))
            state += dotf(k_h, high, over) + dotf(k_h, low, over)
            norm += jnp.sum(k_h.astype(F32) * weight, axis=0, keepdims=True)
            row = base + pairs + h
            xs[x, row : row + 1, :] = jnp.broadcast_to(total, (1, LANES))
            row = base + pairs + heads + h
            xs[x, row : row + 1, :] = jnp.broadcast_to(peak, (1, LANES))
        xs[x, pr * LANES : (pr + 1) * LANES, :] = state
        xs[x, base + pr : base + pr + 1, :] = norm
    spare = p.state_rows - base - pairs - 2 * heads
    if spare:
        xs[x, p.state_rows - spare :, :] = jnp.zeros((spare, LANES), F32)

    def state_x(e):
        return remote(
            xs.at[x], xs.at[x], stx_send.at[e - 1], stx_recv.at[e - 1],
            dev(z, mod(x, e, nx), y, c),
        )

    def state_x_recv(e):
        view = xs.at[mod(x, nx - e, nx)]
        return remote(view, view, stx_send.at[e - 1], stx_recv.at[e - 1], dev(z, mod(x, e, nx), y, c))

    for e in range(1, nx):
        state_x(e).start()

    def join(target, later):
        lo = base + pairs
        tot_e, tot_l = target[lo : lo + heads, :], later[lo : lo + heads, :]
        pk_e = target[lo + heads : lo + 2 * heads, :]
        pk_l = later[lo + heads : lo + 2 * heads, :]
        pk = jnp.maximum(tot_l + pk_e, pk_l)
        w_e, w_l = jnp.exp(tot_l + pk_e - pk), jnp.exp(pk_l - pk)
        for pr in range(pairs):
            hs = [pr * per + i for i in range(per)]
            e_col = jnp.zeros((LANES, LANES), F32)
            l_col = jnp.zeros((LANES, LANES), F32)
            e_row = jnp.zeros((1, LANES), F32)
            l_row = jnp.zeros((1, LANES), F32)
            for i, h in enumerate(hs):
                e_col = jnp.where(subl == i, w_e[h : h + 1, :], e_col)
                l_col = jnp.where(subl == i, w_l[h : h + 1, :], l_col)
                e_row = jnp.where(lane == i, w_e[h : h + 1, :], e_row)
                l_row = jnp.where(lane == i, w_l[h : h + 1, :], l_row)
            blk = slice(pr * LANES, (pr + 1) * LANES)
            target[blk, :] = e_col * target[blk, :] + l_col * later[blk, :]
            row = slice(base + pr, base + pr + 1)
            target[row, :] = e_row * target[row, :] + l_row * later[row, :]
        target[lo : lo + heads, :] = tot_e + tot_l
        target[lo + heads : lo + 2 * heads, :] = pk

    def reset(target):
        target[...] = jnp.zeros((p.state_rows, LANES), F32)
        lo = base + pairs + heads
        target[lo : lo + heads, :] = jnp.full((heads, LANES), -1e30, F32)

    for e in range(1, nx):
        state_x_recv(e).wait_recv()
    mine = zs.at[z]
    reset(mine)
    for i in range(nx):
        join(mine, xs.at[i])

    def state_z(dist):
        return remote(
            zs.at[z], zs.at[z], stz_send.at[dist - 1], stz_recv.at[z],
            dev(lax.rem(z + dist, nz), x, y, c),
        )

    for dist in range(1, nz):
        pl.when(z + dist < nz)(lambda dist=dist: state_z(dist).start())
    for j in range(1, min(EARLY_GROUPS, p.nj)):
        send_group((0, 1), j)

    reset(carry)
    for i in range(nz - 1):

        @pl.when(i < z)
        def _(i=i):
            remote(zs.at[i], zs.at[i], stz_send.at[0], stz_recv.at[i], dev(z, x, y, other)).wait_recv()
            join(carry, zs.at[i])

    for i in range(nx - 1):
        pl.when(i < x)(lambda i=i: join(carry, xs.at[i]))

    lo = base + pairs
    total_in = carry[lo : lo + heads, :]
    peak_raw = carry[lo + heads : lo + 2 * heads, :]
    peak_all = jnp.maximum(peak_raw, total_in)
    scale_all = jnp.exp(peak_raw - peak_all)
    unit = p.qk ** (-0.5)
    qrows = min(QUERY_ROWS, tok)
    for h in range(heads):
        pr = h // per
        peak_in = peak_all[h : h + 1, 0:1]
        scale = scale_all[h : h + 1, :]
        st_high, st_low = split(carry[pr * LANES : (pr + 1) * LANES, :] * scale)
        norm_in = carry[base + pr : base + pr + 1, :] * scale
        k2 = keys[:, pr * LANES : (pr + 1) * LANES]
        v_h = values[:, h * p.vd : (h + 1) * p.vd]
        for r0 in range(0, tok, qrows):
            r1 = r0 + qrows
            q2 = queries[r0:r1, pr * LANES : (pr + 1) * LANES]
            q_h = jnp.where(lane == h % per, q2, jnp.zeros_like(q2))
            cum_c = col[r0:r1, h : h + 1]
            seen = (
                lax.broadcasted_iota(jnp.int32, (qrows, r1), 0) + r0
                >= lax.broadcasted_iota(jnp.int32, (qrows, r1), 1)
            )
            logs = jnp.where(seen, bias_row[h : h + 1, :r1], -jnp.inf) + cum_c
            inter = cum_c + peak_in
            peak_row = jnp.maximum(inter, jnp.max(logs, axis=1, keepdims=True))
            dots = dotf(q_h, k2[:r1], (((1,), (1,)), ((), ()))) * unit
            probs = dots * jnp.exp(logs - peak_row)
            inter_scale = jnp.exp(inter - peak_row) * unit
            high, low = split(probs)
            numer = dotf(high, v_h[:r1]) + dotf(low, v_h[:r1])
            numer += inter_scale * (dotf(q_h, st_high) + dotf(q_h, st_low))
            denom = jnp.sum(probs, axis=1, keepdims=True) + inter_scale * jnp.sum(
                q_h.astype(F32) * norm_in, axis=1, keepdims=True
            )
            cell = numer / jnp.maximum(jnp.abs(denom), jnp.exp(-peak_row))
            square = jnp.mean(cell * cell, axis=1, keepdims=True)
            span = slice(h * p.vd, (h + 1) * p.vd)
            gain = head_gain[:, span].astype(F32)
            gates = jax.nn.sigmoid(out_gate[r0:r1, span].astype(F32))
            gated[r0:r1, span] = (cell * lax.rsqrt(square + 1e-06) * gain * gates).astype(BF16)

    relay((0, 1), 0)

    pieces = p.d // p.wc

    def fetch_w(n):
        return pltpu.make_async_copy(
            out_w.at[:, pl.ds(n * p.wc, p.wc)],
            slab.at[n % 2, pl.ds(0, p.vw), pl.ds(0, p.wc)],
            local.at[n % 2],
        )

    fetch_w(0).start()
    for n in range(pieces):
        if n + 1 < pieces:
            fetch_w(n + 1).start()
        fetch_w(n).wait()
        for c0 in range(0, p.wc, p.cc):
            g0 = n * p.wc + c0
            w = slab[n % 2, : p.vw, c0 : c0 + p.cc]
            res_ = dotf(gated[...], w).astype(BF16)
            for b in range(p.tp):
                parts[g0 // p.cw, b // ny, b % ny, :, g0 % p.cw : g0 % p.cw + p.cc] = res_[
                    b * p.own : (b + 1) * p.own
                ]

    cols_used = p.d // p.cw

    def at_peer(yy):
        b = yy * nc + other
        return remote(
            parts.at[pl.ds(0, cols_used), b // ny, lax.rem(b, ny)],
            cr.at[:, yy], at_send.at[yy], at_recv.at[yy], dev(z, x, y, other),
        )

    for yy in range(ny):
        at_peer(yy).start()
    relay((0, 1), 1)

    def at_y(e):
        b = mod(y, e, ny) * nc + c
        return remote(
            parts.at[pl.ds(0, cols_used), b // ny, lax.rem(b, ny)],
            yr.at[:, e - 1], ay_send.at[e - 1], ay_recv.at[e - 1], dev(z, x, mod(y, e, ny), c),
        )

    for yy in range(ny):
        at_peer(yy).wait_recv()
    for e in range(1, ny):
        to = mod(y, e, ny)
        b = to * nc + c
        for n in range(cols_used):
            parts[n, b // ny, lax.rem(b, ny)] = (
                parts[n, b // ny, lax.rem(b, ny)].astype(F32) + cr[n, to].astype(F32)
            ).astype(BF16)
        at_y(e).start()
    fetch_res.wait()
    b = y * nc + c
    for n in range(cols_used):
        cols = slice(n * p.cw, (n + 1) * p.cw)
        stream[:, cols] = (
            res[:, cols].astype(F32)
            + parts[n, b // ny, lax.rem(b, ny)].astype(F32) + cr[n, y].astype(F32)
        )
    settle((0, 1), 0)
    for e in range(1, ny):
        at_y(e).wait_recv()
        for n in range(cols_used):
            cols = slice(n * p.cw, (n + 1) * p.cw)
            stream[:, cols] += yr[n, e - 1].astype(F32)
    cut = p.own // GATHER_CUTS
    for s in range(GATHER_CUTS):
        rows = slice(s * cut, (s + 1) * cut)
        part = stream[rows, :]
        square = jnp.mean(part * part, axis=1, keepdims=True)
        tokens[z, y, rows, :] = (
            part * lax.rsqrt(square + 1e-06) * ff_gain[...].astype(F32)
        ).astype(BF16)

    def block(zz, yy, s):
        return tokens.at[zz, yy, pl.ds(s * cut, cut), :]

    def go_right(zz, s):
        return remote(block(zz, y, s), block(zz, y, s), gz_right.at[zz, s], gz_recv.at[zz, s],
                      dev(z + 1, x, y, c))

    def go_left(zz, s):
        return remote(block(zz, y, s), block(zz, y, s), gz_left.at[zz, s], gz_recv.at[zz, s],
                      dev(z - 1, x, y, c))

    def go_y(zz, s, e):
        return remote(block(zz, y, s), block(zz, y, s), gy_send.at[zz, s, e - 1],
                      gy_recv.at[zz, s, e - 1], dev(z, x, mod(y, e, ny), c))

    def y_recv(zz, s, e):
        view = block(zz, mod(y, ny - e, ny), s)
        return remote(view, view, gy_send.at[zz, s, e - 1], gy_recv.at[zz, s, e - 1],
                      dev(z, x, mod(y, e, ny), c))

    for s in range(GATHER_CUTS):
        pl.when(z + 1 < nz)(lambda s=s: go_right(z, s).start())
        pl.when(z >= 1)(lambda s=s: go_left(z, s).start())
        for e in range(1, ny):
            go_y(z, s, e).start()
    for dist in range(1, nz):
        for s in range(GATHER_CUTS):

            @pl.when(z - dist >= 0)
            def _(dist=dist, s=s):
                go_right(z - dist, s).wait_recv()
                pl.when(z + 1 < nz)(lambda: go_right(z - dist, s).start())
                for e in range(1, ny):
                    go_y(z - dist, s, e).start()

            @pl.when(z + dist < nz)
            def _(dist=dist, s=s):
                go_left(z + dist, s).wait_recv()
                pl.when(z >= 1)(lambda: go_left(z + dist, s).start())
                for e in range(1, ny):
                    go_y(z + dist, s, e).start()

        if dist == 1:
            relay((0, 1), 2 % p.nj) if p.nj > 2 else None
    for j in range(min(EARLY_GROUPS, p.nj), p.nj):
        send_group((0, 1), j)
    for j in range(p.nj):
        send_group((2,), j)
    for j in range(1, min(3, p.nj)):
        settle((0, 1), j)
    for zz in range(nz):
        for s in range(GATHER_CUTS):
            for e in range(1, ny):
                y_recv(zz, s, e).wait_recv()
    for s in range(GATHER_CUTS):

        def sent(zz, s=s):
            pl.when((z + 1 < nz) & (zz <= z))(lambda: go_right(zz, s).wait_send())
            pl.when((z >= 1) & (zz >= z))(lambda: go_left(zz, s).wait_send())
            for e in range(1, ny):
                go_y(zz, s, e).wait_send()

        for zz in range(nz):
            sent(zz)

    trows = p.ny * p.own

    def load_slab(m, j):
        return [
            pltpu.make_async_copy(
                mats[m][1].at[s, jrows(j), :],
                slab.at[m, pl.ds(s * LANES, LANES), :],
                local.at[m],
            )
            for s in range(p.sp)
        ]

    def whole_slab(m):
        return pltpu.make_async_copy(slab.at[m], slab.at[m], local.at[m])

    for j in range(p.nj):
        if j >= 3:
            relay((0, 1), j)
            settle((0, 1), j)
        for m in range(2):
            for copy in load_slab(m, j):
                copy.start()
        for m in range(2):
            whole_slab(m).wait()

        @pl.loop(0, nz)
        def _(zz, j=j):
            lhs = jnp.concatenate(
                [
                    tokens[zz, :, :, s * p.rows + j * LANES : s * p.rows + (j + 1) * LANES].reshape(
                        trows, LANES
                    )
                    for s in range(p.sp)
                ],
                axis=1,
            )
            for m in range(2):
                more = dotf(lhs, slab[m])
                if j == 0:
                    acc[zz, m] = more
                else:
                    acc[zz, m] += more

    @pl.loop(0, nz)
    def _(zz):
        hidden = jax.nn.silu(acc[zz, 0]) * acc[zz, 1]
        if any(p.dup):
            seen_col = lax.broadcasted_iota(jnp.int32, (1, p.hid), 1)
            for i in range(p.zc):
                if p.dup[i]:
                    drop = (seen_col < p.dup[i]) & (lax.rem(z, p.zc) == i)
                    hidden = jnp.where(drop, 0.0, hidden)
        tokens[zz, :, :, : p.hid] = hidden.astype(BF16).reshape(ny, p.own, p.hid)

    def ry(n, e):
        return remote(
            parts.at[n, :, mod(y, e, ny)], yb.at[n, e - 1], ry_send.at[n, e - 1],
            ry_recv.at[n, e - 1], dev(z, x, mod(y, e, ny), c),
        )

    def rz_right(n, o):
        return remote(parts.at[n, o, y], lb.at[n, o - 1], rr_send.at[n, o], rl_recv.at[n, o],
                      dev(z + 1, x, y, c))

    def rz_left(n, o):
        return remote(parts.at[n, o, y], rb.at[n, o], rl_send.at[n, o], rr_recv.at[n, o],
                      dev(z - 1, x, y, c))

    for yy in range(ny):
        at_peer(yy).wait_send()
    for e in range(1, ny):
        at_y(e).wait_send()

    def add_stream(n, more):
        j, half = n // p.halves, lax.rem(n, p.halves)
        for q in range(p.sph):
            at = pl.multiple_of((half * p.sph + q) * p.rows + j * LANES, LANES)
            stream[:, pl.ds(at, LANES)] += 0.5 * more[:, q * LANES : (q + 1) * LANES]

    def load_down(n):
        j, half = n // p.halves, lax.rem(n, p.halves)
        return [
            pltpu.make_async_copy(
                down_b.at[half * p.sph + q, jrows(j), :],
                slab.at[0, pl.ds(q * LANES, LANES), :],
                local.at[0],
            )
            for q in range(p.sph)
        ]

    def step(i, _):
        @pl.when(i < p.ns)
        def _():
            j = i // p.halves

            @pl.when(lax.rem(i, p.halves) == 0)
            def _():
                relay((2,), j)
                settle((2,), j)

            for copy in load_down(i):
                copy.start()
            view = slab.at[0, pl.ds(0, p.sph * LANES), :]
            pltpu.make_async_copy(view, view, local.at[0]).wait()

            @pl.loop(0, nz)
            def _(zz):
                hid = tokens[zz, :, :, : p.hid].reshape(trows, p.hid)
                terms = dotf(hid, slab[0, : p.sph * LANES, :], (((1,), (1,)), ((), ())))
                parts[i, zz] = terms.astype(BF16).reshape(ny, p.own, p.cw)

            for e in range(1, ny):
                ry(i, e).start()

        @pl.when((i >= 1) & (i <= p.ns))
        def _():
            n = i - 1
            for e in range(1, ny):
                ry(n, e).wait_recv()

            @pl.loop(0, nz)
            def _(o):
                total = parts[n, o, y].astype(F32)
                for e in range(1, ny):
                    total += yb[n, e - 1, o].astype(F32)
                parts[n, o, y] = total.astype(BF16)
                pl.when(o == z)(lambda: add_stream(n, total))

        right = i - 1 - z

        @pl.when((right >= 0) & (right < p.ns))
        def _():
            for o in range(1, nz):

                @pl.when((o >= z) & (z > 0))
                def _(o=o):
                    rz_right(right, o).wait_recv()

                @pl.when((o > z) & (z > 0))
                def _(o=o):
                    parts[right, o, y] = (
                        parts[right, o, y].astype(F32) + lb[right, o - 1].astype(F32)
                    ).astype(BF16)

                pl.when(o > z)(lambda o=o: rz_right(right, o).start())
                pl.when(o == z)(lambda o=o: add_stream(right, lb[right, o - 1].astype(F32)))

        left = i - 1 - (nz - 1 - z)

        @pl.when((left >= 0) & (left < p.ns))
        def _():
            for o in range(nz - 1):

                @pl.when((o <= z) & (z < nz - 1))
                def _(o=o):
                    rz_left(left, o).wait_recv()

                @pl.when((o < z) & (z < nz - 1))
                def _(o=o):
                    parts[left, o, y] = (
                        parts[left, o, y].astype(F32) + rb[left, o].astype(F32)
                    ).astype(BF16)

                pl.when(o < z)(lambda o=o: rz_left(left, o).start())
                pl.when(o == z)(lambda o=o: add_stream(left, rb[left, o].astype(F32)))

        return 0

    lax.fori_loop(0, p.ns + nz, step, 0)
    out[...] = stream[...].astype(BF16)

    for e in range(1, nx):
        state_x(e).wait_send()
    for dist in range(1, nz):
        pl.when(z + dist < nz)(lambda dist=dist: state_z(dist).wait_send())

    @pl.loop(0, p.nj)
    def _(j):
        for m in range(3):
            for i in range(p.zc):
                first_hop(m, j, i).wait_send()

            @pl.when(duty)
            def _(m=m):
                for zz in range(nz):
                    for e in range(1, nx):
                        across(m, j, zz, e).wait_send()
                peer_all(m, j).wait_send()

    @pl.loop(0, p.ns)
    def _(n):
        for e in range(1, ny):
            ry(n, e).wait_send()
        for o in range(nz):
            if o:
                pl.when(o > z)(lambda o=o: rz_right(n, o).wait_send())
            if o < nz - 1:
                pl.when(o < z)(lambda o=o: rz_left(n, o).wait_send())


def solution(mesh):
    def per_device(*args):
        (residual, queries, keys, values, out_gate, in_gate, forget, extra, head_gain, out_w,
         ff_gain, gate_w, up_w, down_w) = args
        p = Plan(
            dict(mesh.shape),
            {
                "residual": residual.shape, "queries": queries.shape, "values": values.shape,
                "gates": in_gate.shape, "gate": gate_w.shape,
            },
        )
        vmem = pl.BlockSpec(memory_space=pltpu.VMEM)
        hbm = pl.BlockSpec(memory_space=pl.ANY)
        dma = pltpu.SemaphoreType.DMA
        held = jax.ShapeDtypeStruct((p.sp, p.rows, p.hid), BF16)
        nj, nz, nx, ny, ns = p.nj, p.nz, p.nx, p.ny, p.ns
        cols_used = p.d // p.cw
        cols8 = -(-2 * p.heads // 8) * 8
        scratch = [
            pltpu.VMEM((p.tok, cols8), F32),
            pltpu.VMEM((p.tok, p.vw), BF16),
            pltpu.VMEM((nx, p.state_rows, LANES), F32),
            pltpu.VMEM((nz, p.state_rows, LANES), F32),
            pltpu.VMEM((p.state_rows, LANES), F32),
            pltpu.VMEM((nz, ny, p.own, p.d), BF16),
            pltpu.VMEM((nz, 2, ny * p.own, p.hid), F32),
            pltpu.VMEM((2, p.sp * LANES, p.hid), BF16),
            pltpu.VMEM((ns, nz, ny, p.own, p.cw), BF16),
            pltpu.VMEM((ns, ny - 1, nz, p.own, p.cw), BF16),
            pltpu.VMEM((ns, nz - 1, p.own, p.cw), BF16),
            pltpu.VMEM((ns, nz - 1, p.own, p.cw), BF16),
            pltpu.VMEM((p.own, p.d), F32),
            pltpu.VMEM((cols_used, ny, p.own, p.cw), BF16),
            pltpu.VMEM((cols_used, ny - 1, p.own, p.cw), BF16),
            pltpu.VMEM((p.own, p.d), BF16),
            dma((3, nj, p.zc)), dma((3, nj, nz)),
            dma((3, nj, nz, nx - 1)), dma((3, nj, nz, nx - 1)),
            dma((3, nj)), dma((3, nj)),
            dma((nx - 1,)), dma((nx - 1,)),
            dma((nz - 1,)), dma((nz,)),
            dma((ny,)), dma((ny,)), dma((ny - 1,)), dma((ny - 1,)),
            dma((nz, GATHER_CUTS)), dma((nz, GATHER_CUTS)), dma((nz, GATHER_CUTS)),
            dma((nz, GATHER_CUTS, ny - 1)), dma((nz, GATHER_CUTS, ny - 1)),
            dma((ns, ny - 1)), dma((ns, ny - 1)),
            dma((ns, nz)), dma((ns, nz)), dma((ns, nz)), dma((ns, nz)),
            dma((3,)),
        ]
        result = pl.pallas_call(
            functools.partial(layer, p),
            out_shape=(
                jax.ShapeDtypeStruct((p.own, p.d), BF16), held, held, held,
            ),
            in_specs=[hbm] + [vmem] * 8 + [hbm, vmem] + [hbm] * 3,
            out_specs=(vmem, hbm, hbm, hbm),
            scratch_shapes=scratch,
            compiler_params=pltpu.CompilerParams(
                collective_id=0, has_side_effects=True, vmem_limit_bytes=67043328
            ),
            name="layer",
        )(
            residual, queries, keys, values, out_gate, in_gate, forget, extra,
            head_gain.reshape(1, -1), out_w, ff_gain.reshape(1, -1), gate_w, up_w, down_w,
        )
        return result[0]

    in_specs = (
        P("sp", None), P("sp", "tp"), P("sp", "tp"), P("sp", "tp"), P("sp", "tp"),
        P("tp", "sp"), P("tp", "sp"), P("tp", "sp"), P("tp"), P("tp", None), P(),
        P("sp", "tp"), P("sp", "tp"), P("sp", "tp"),
    )
    return jax.shard_map(
        per_device, mesh=mesh, in_specs=in_specs, out_specs=P(("sp", "tp"), None), check_vma=False
    )
```

```python
import functools
import jax
import jax.numpy as jnp
from jax import lax
from jax.experimental import pallas as pl
from jax.experimental.pallas import tpu as pltpu
from jax.sharding import PartitionSpec as P

MESH = pl.DeviceIdType.MESH
F32 = jnp.float32
BF16 = jnp.bfloat16
LANES = 128
QUERY_ROWS = 256
TOKEN_ROWS = 256
GATHER_CUTS = 2
EARLY_GROUPS = 2


class Plan:
    def __init__(self, mesh_shape, shapes):
        self.sp, self.tp = mesh_shape["sp"], mesh_shape["tp"]
        self.nz = next(n for n in range(1, self.sp + 1) if self.sp % n == 0 and n * n >= self.sp)
        self.nx = self.sp // self.nz
        self.nc = 2
        self.ny = self.tp // self.nc
        self.tok, self.d = shapes["residual"]
        self.own = self.tok // self.tp
        self.heads = shapes["gates"][0]
        self.qk = shapes["queries"][1] // self.heads
        self.vd = shapes["values"][1] // self.heads
        self.per = LANES // self.qk
        self.pairs = self.heads // self.per
        self.vw = shapes["values"][1]
        self.rows, self.ff = shapes["gate"]
        self.zc = self.nz // self.nc
        tiles = self.ff // LANES
        wide = -(-tiles // self.zc)
        starts = [min(i * wide, tiles - wide) for i in range(self.zc)]
        self.start = [s * LANES for s in starts]
        self.dup = [(i * wide - s) * LANES for i, s in enumerate(starts)]
        self.hid = wide * LANES
        self.nj = self.rows // LANES
        self.halves = 2
        self.sph = self.sp // self.halves
        self.cw = self.sph * LANES
        self.ns = self.nj * self.halves
        self.toks = self.nz * self.ny * self.own
        self.state_rows = self.pairs * LANES + -(-(self.pairs + 2 * self.heads) // 8) * 8
        self.wc = next(
            n for n in range(self.hid // LANES * LANES, 0, -LANES) if self.d % n == 0
        )
        self.cc = min(self.cw, self.wc)


def dotf(a, b, dims=(((1,), (0,)), ((), ())), precision=None):
    return lax.dot_general(a, b, dims, preferred_element_type=F32, precision=precision)


def split(a):
    high = a.astype(BF16)
    return high, (a - high.astype(F32)).astype(BF16)


def layer(p, *refs):
    (
        residual, queries, keys, values, out_gate, in_gate, forget, extra, head_gain, out_w,
        ff_gain, gate_w, up_w, down_w,
        out, gate_b, up_b, down_b,
        col, gated, xs, zs, carry, tokens, acc, slab, parts, yb, lb, rb, stream, cr, yr, res,
        s1_send, s1_recv, xf_send, xf_recv, pf_send, pf_recv,
        stx_send, stx_recv, stz_send, stz_recv, at_send, at_recv, ay_send, ay_recv,
        gz_right, gz_left, gz_recv, gy_send, gy_recv,
        ry_send, ry_recv, rr_send, rl_send, rl_recv, rr_recv, local,
    ) = refs
    nz, nx, ny, nc = p.nz, p.nx, p.ny, p.nc
    sp_i, tp_i = lax.axis_index("sp"), lax.axis_index("tp")
    z, x = sp_i // nx, lax.rem(sp_i, nx)
    y, c = tp_i // nc, lax.rem(tp_i, nc)
    other = 1 - c
    duty = c == 1 - z // p.zc

    def dev(z_, x_, y_, c_):
        return (z_ * nx + x_, y_ * nc + c_)

    def mod(a, e, n):
        return lax.rem(a + e, n)

    def remote(src, dst, send, recv, device):
        return pltpu.make_async_remote_copy(
            src_ref=src, dst_ref=dst, send_sem=send, recv_sem=recv,
            device_id=device, device_id_type=MESH,
        )

    barrier = pltpu.get_barrier_semaphore()
    friends = [dev(mod(z, e, nz), x, y, c) for e in range(1, nz)]
    friends += [dev(z, mod(x, e, nx), y, c) for e in range(1, nx)]
    friends += [dev(z, x, mod(y, e, ny), c) for e in range(1, ny)]
    friends += [dev(mod(z, e, nz), x, y, other) for e in range(nz)]
    for friend in friends:
        pl.semaphore_signal(barrier, inc=1, device_id=friend, device_id_type=MESH)
    pl.semaphore_wait(barrier, len(friends))

    mats = ((gate_w, gate_b), (up_w, up_b), (down_w, down_b))

    def jrows(j):
        return pl.ds(pl.multiple_of(j * LANES, LANES), LANES)

    def first_hop(m, j, i):
        src, dst = mats[m]
        return remote(
            src.at[jrows(j), pl.ds(p.start[i], p.hid)],
            dst.at[sp_i, jrows(j), :],
            s1_send.at[m, j, i], s1_recv.at[m, j, z],
            dev(c * p.zc + i, x, y, other),
        )

    def first_recv(m, j, zs_):
        src, dst = mats[m]
        view = dst.at[zs_ * nx + x, jrows(j), :]
        return remote(view, view, s1_send.at[m, j, 0], s1_recv.at[m, j, zs_], dev(z, x, y, other))

    def across(m, j, zs_, e):
        view = mats[m][1].at[zs_ * nx + x, jrows(j), :]
        return remote(
            view, view, xf_send.at[m, j, zs_, e - 1], xf_recv.at[m, j, zs_, e - 1],
            dev(z, mod(x, e, nx), y, c),
        )

    def across_recv(m, j, zs_, e):
        view = mats[m][1].at[zs_ * nx + mod(x, nx - e, nx), jrows(j), :]
        return remote(
            view, view, xf_send.at[m, j, zs_, e - 1], xf_recv.at[m, j, zs_, e - 1],
            dev(z, mod(x, e, nx), y, c),
        )

    def to_peer(m, j, sp_):
        view = mats[m][1].at[sp_, jrows(j), :]
        return remote(view, view, pf_send.at[m, j], pf_recv.at[m, j], dev(z, x, y, other))

    def peer_all(m, j):
        view = mats[m][1].at[:, jrows(j), :]
        return remote(view, view, pf_send.at[m, j], pf_recv.at[m, j], dev(z, x, y, other))

    def send_group(ms, j):
        for i in range(p.zc):

            @pl.when(c * p.zc + i != z)
            def _(i=i):
                for m in ms:
                    first_hop(m, j, i).start()

    def send_own():
        for i in range(p.zc):

            @pl.when(c * p.zc + i == z)
            def _(i=i):
                for m in range(3):
                    for j in range(p.nj):
                        first_hop(m, j, i).start()

    def each_other(fn):
        for dist in range(1, nz):
            pl.when(z - dist >= 0)(functools.partial(fn, z - dist))
            pl.when(z + dist < nz)(functools.partial(fn, z + dist))

    def each_z(fn):
        fn(z)
        each_other(fn)

    def pass_on(ms, j, zs_):
        for m in ms:
            first_recv(m, j, zs_).wait_recv()
            for e in range(1, nx):
                across(m, j, zs_, e).start()
            to_peer(m, j, zs_ * nx + x).start()

    def relay(ms, j):
        @pl.when(duty)
        def _():
            each_other(functools.partial(pass_on, ms, j))

    def relay_own(ms):
        @pl.when(duty)
        def _():
            for j in range(p.nj):
                pass_on(ms, j, z)

    def settle(ms, j):
        @pl.when(duty)
        def _():
            def one(zs_):
                for m in ms:
                    for e in range(1, nx):
                        across_recv(m, j, zs_, e).wait_recv()
                        to_peer(m, j, zs_ * nx + mod(x, nx - e, nx)).start()

            each_z(one)

        @pl.when(jnp.logical_not(duty))
        def _():
            for m in ms:
                peer_all(m, j).wait_recv()

    send_group((0,), 0)
    send_own()
    fetch_res = pltpu.make_async_copy(
        residual.at[pl.ds(pl.multiple_of(tp_i * p.own, p.own), p.own), :], res, local.at[2]
    )
    fetch_res.start()

    heads, per, pairs, tok = p.heads, p.per, p.pairs, p.tok
    fg = forget[...]
    lf = jnp.minimum(fg, 0.0) - jnp.log1p(jnp.exp(-jnp.abs(fg))) + extra[...]
    upper = (
        lax.broadcasted_iota(jnp.int32, (tok, tok), 0)
        <= lax.broadcasted_iota(jnp.int32, (tok, tok), 1)
    ).astype(F32)
    pad = jnp.zeros((-heads % 8, tok), F32)
    lf8 = jnp.concatenate([lf, pad], axis=0) if pad.shape[0] else lf
    cum_row = dotf(lf8, upper, precision=lax.Precision.HIGHEST)[:heads]
    ig = in_gate[...]
    pad = jnp.zeros((-2 * heads % 8, tok), F32)
    both = [cum_row, ig] + ([pad] if pad.shape[0] else [])
    col[...] = jnp.concatenate(both, axis=0).T
    bias_row = ig - cum_row
    base = pairs * LANES
    lane = lax.broadcasted_iota(jnp.int32, (1, LANES), 1) // p.qk
    subl = lax.broadcasted_iota(jnp.int32, (LANES, 1), 0) // p.qk

    def head_lanes(ref, h):
        pair = ref[:, h // per * LANES : (h // per + 1) * LANES]
        return jnp.where(lane == h % per, pair, jnp.zeros_like(pair))

    for pr in range(pairs):
        state = jnp.zeros((LANES, LANES), F32)
        norm = jnp.zeros((1, LANES), F32)
        for h in range(pr * per, (pr + 1) * per):
            total = cum_row[h : h + 1, tok - 1 : tok]
            log_w = total - col[:, h : h + 1] + col[:, heads + h : heads + h + 1]
            peak = jnp.max(log_w, axis=0, keepdims=True)
            weight = jnp.exp(log_w - peak)
            k_h = head_lanes(keys, h)
            high, low = split(values[:, h * p.vd : (h + 1) * p.vd].astype(F32) * weight)
            over = (((0,), (0,)), ((), ()))
            state += dotf(k_h, high, over) + dotf(k_h, low, over)
            norm += jnp.sum(k_h.astype(F32) * weight, axis=0, keepdims=True)
            row = base + pairs + h
            xs[x, row : row + 1, :] = jnp.broadcast_to(total, (1, LANES))
            row = base + pairs + heads + h
            xs[x, row : row + 1, :] = jnp.broadcast_to(peak, (1, LANES))
        xs[x, pr * LANES : (pr + 1) * LANES, :] = state
        xs[x, base + pr : base + pr + 1, :] = norm
    spare = p.state_rows - base - pairs - 2 * heads
    if spare:
        xs[x, p.state_rows - spare :, :] = jnp.zeros((spare, LANES), F32)

    def state_x(e):
        return remote(
            xs.at[x], xs.at[x], stx_send.at[e - 1], stx_recv.at[e - 1],
            dev(z, mod(x, e, nx), y, c),
        )

    def state_x_recv(e):
        view = xs.at[mod(x, nx - e, nx)]
        return remote(view, view, stx_send.at[e - 1], stx_recv.at[e - 1], dev(z, mod(x, e, nx), y, c))

    for e in range(1, nx):
        state_x(e).start()

    def join(target, later):
        lo = base + pairs
        tot_e, tot_l = target[lo : lo + heads, :], later[lo : lo + heads, :]
        pk_e = target[lo + heads : lo + 2 * heads, :]
        pk_l = later[lo + heads : lo + 2 * heads, :]
        pk = jnp.maximum(tot_l + pk_e, pk_l)
        w_e, w_l = jnp.exp(tot_l + pk_e - pk), jnp.exp(pk_l - pk)
        for pr in range(pairs):
            hs = [pr * per + i for i in range(per)]
            e_col = jnp.zeros((LANES, LANES), F32)
            l_col = jnp.zeros((LANES, LANES), F32)
            e_row = jnp.zeros((1, LANES), F32)
            l_row = jnp.zeros((1, LANES), F32)
            for i, h in enumerate(hs):
                e_col = jnp.where(subl == i, w_e[h : h + 1, :], e_col)
                l_col = jnp.where(subl == i, w_l[h : h + 1, :], l_col)
                e_row = jnp.where(lane == i, w_e[h : h + 1, :], e_row)
                l_row = jnp.where(lane == i, w_l[h : h + 1, :], l_row)
            blk = slice(pr * LANES, (pr + 1) * LANES)
            target[blk, :] = e_col * target[blk, :] + l_col * later[blk, :]
            row = slice(base + pr, base + pr + 1)
            target[row, :] = e_row * target[row, :] + l_row * later[row, :]
        target[lo : lo + heads, :] = tot_e + tot_l
        target[lo + heads : lo + 2 * heads, :] = pk

    def reset(target):
        target[...] = jnp.zeros((p.state_rows, LANES), F32)
        lo = base + pairs + heads
        target[lo : lo + heads, :] = jnp.full((heads, LANES), -1e30, F32)

    for e in range(1, nx):
        state_x_recv(e).wait_recv()
    mine = zs.at[z]
    reset(mine)
    for i in range(nx):
        join(mine, xs.at[i])

    def state_z(dist):
        return remote(
            zs.at[z], zs.at[z], stz_send.at[dist - 1], stz_recv.at[z],
            dev(lax.rem(z + dist, nz), x, y, c),
        )

    for dist in range(1, nz):
        pl.when(z + dist < nz)(lambda dist=dist: state_z(dist).start())
    send_group((1,), 0)
    for j in range(1, min(EARLY_GROUPS, p.nj)):
        send_group((0, 1), j)
    relay_own((0, 1))

    reset(carry)
    for i in range(nz - 1):

        @pl.when(i < z)
        def _(i=i):
            remote(zs.at[i], zs.at[i], stz_send.at[0], stz_recv.at[i], dev(z, x, y, other)).wait_recv()
            join(carry, zs.at[i])

    for i in range(nx - 1):
        pl.when(i < x)(lambda i=i: join(carry, xs.at[i]))

    lo = base + pairs
    total_in = carry[lo : lo + heads, :]
    peak_raw = carry[lo + heads : lo + 2 * heads, :]
    peak_all = jnp.maximum(peak_raw, total_in)
    scale_all = jnp.exp(peak_raw - peak_all)
    unit = p.qk ** (-0.5)
    qrows = min(QUERY_ROWS, tok)
    for h in range(heads):
        pr = h // per
        peak_in = peak_all[h : h + 1, 0:1]
        scale = scale_all[h : h + 1, :]
        st_high, st_low = split(carry[pr * LANES : (pr + 1) * LANES, :] * scale)
        norm_in = carry[base + pr : base + pr + 1, :] * scale
        k2 = keys[:, pr * LANES : (pr + 1) * LANES]
        v_h = values[:, h * p.vd : (h + 1) * p.vd]
        for r0 in range(0, tok, qrows):
            r1 = r0 + qrows
            q2 = queries[r0:r1, pr * LANES : (pr + 1) * LANES]
            q_h = jnp.where(lane == h % per, q2, jnp.zeros_like(q2))
            cum_c = col[r0:r1, h : h + 1]
            seen = (
                lax.broadcasted_iota(jnp.int32, (qrows, r1), 0) + r0
                >= lax.broadcasted_iota(jnp.int32, (qrows, r1), 1)
            )
            logs = jnp.where(seen, bias_row[h : h + 1, :r1], -jnp.inf) + cum_c
            inter = cum_c + peak_in
            peak_row = jnp.maximum(inter, jnp.max(logs, axis=1, keepdims=True))
            dots = dotf(q_h, k2[:r1], (((1,), (1,)), ((), ()))) * unit
            probs = dots * jnp.exp(logs - peak_row)
            inter_scale = jnp.exp(inter - peak_row) * unit
            high, low = split(probs)
            numer = dotf(high, v_h[:r1]) + dotf(low, v_h[:r1])
            numer += inter_scale * (dotf(q_h, st_high) + dotf(q_h, st_low))
            denom = jnp.sum(probs, axis=1, keepdims=True) + inter_scale * jnp.sum(
                q_h.astype(F32) * norm_in, axis=1, keepdims=True
            )
            cell = numer / jnp.maximum(jnp.abs(denom), jnp.exp(-peak_row))
            square = jnp.mean(cell * cell, axis=1, keepdims=True)
            span = slice(h * p.vd, (h + 1) * p.vd)
            gain = head_gain[:, span].astype(F32)
            gates = jax.nn.sigmoid(out_gate[r0:r1, span].astype(F32))
            gated[r0:r1, span] = (cell * lax.rsqrt(square + 1e-06) * gain * gates).astype(BF16)

    pieces = p.d // p.wc

    def fetch_w(n):
        return pltpu.make_async_copy(
            out_w.at[:, pl.ds(n * p.wc, p.wc)],
            slab.at[n % 2, pl.ds(0, p.vw), pl.ds(0, p.wc)],
            local.at[n % 2],
        )

    fetch_w(0).start()
    for n in range(pieces):
        if n + 1 < pieces:
            fetch_w(n + 1).start()
        fetch_w(n).wait()
        for c0 in range(0, p.wc, p.cc):
            g0 = n * p.wc + c0
            w = slab[n % 2, : p.vw, c0 : c0 + p.cc]
            res_ = dotf(gated[...], w).astype(BF16)
            for b in range(p.tp):
                parts[g0 // p.cw, b // ny, b % ny, :, g0 % p.cw : g0 % p.cw + p.cc] = res_[
                    b * p.own : (b + 1) * p.own
                ]

    cols_used = p.d // p.cw

    def at_peer(yy):
        b = yy * nc + other
        return remote(
            parts.at[pl.ds(0, cols_used), b // ny, lax.rem(b, ny)],
            cr.at[:, yy], at_send.at[yy], at_recv.at[yy], dev(z, x, y, other),
        )

    for yy in range(ny):
        at_peer(yy).start()

    def at_y(e):
        b = mod(y, e, ny) * nc + c
        return remote(
            parts.at[pl.ds(0, cols_used), b // ny, lax.rem(b, ny)],
            yr.at[:, e - 1], ay_send.at[e - 1], ay_recv.at[e - 1], dev(z, x, mod(y, e, ny), c),
        )

    for yy in range(ny):
        at_peer(yy).wait_recv()
    for e in range(1, ny):
        to = mod(y, e, ny)
        b = to * nc + c
        for n in range(cols_used):
            parts[n, b // ny, lax.rem(b, ny)] = (
                parts[n, b // ny, lax.rem(b, ny)].astype(F32) + cr[n, to].astype(F32)
            ).astype(BF16)
        at_y(e).start()
    fetch_res.wait()
    b = y * nc + c
    for n in range(cols_used):
        cols = slice(n * p.cw, (n + 1) * p.cw)
        stream[:, cols] = (
            res[:, cols].astype(F32)
            + parts[n, b // ny, lax.rem(b, ny)].astype(F32) + cr[n, y].astype(F32)
        )
    relay((0, 1), 0)
    for e in range(1, ny):
        at_y(e).wait_recv()
        for n in range(cols_used):
            cols = slice(n * p.cw, (n + 1) * p.cw)
            stream[:, cols] += yr[n, e - 1].astype(F32)
    cut = p.own // GATHER_CUTS
    for s in range(GATHER_CUTS):
        rows = slice(s * cut, (s + 1) * cut)
        part = stream[rows, :]
        square = jnp.mean(part * part, axis=1, keepdims=True)
        tokens[z, y, rows, :] = (
            part * lax.rsqrt(square + 1e-06) * ff_gain[...].astype(F32)
        ).astype(BF16)

    def block(zz, yy, s):
        return tokens.at[zz, yy, pl.ds(s * cut, cut), :]

    def go_right(zz, s):
        return remote(block(zz, y, s), block(zz, y, s), gz_right.at[zz, s], gz_recv.at[zz, s],
                      dev(z + 1, x, y, c))

    def go_left(zz, s):
        return remote(block(zz, y, s), block(zz, y, s), gz_left.at[zz, s], gz_recv.at[zz, s],
                      dev(z - 1, x, y, c))

    def go_y(zz, s, e):
        return remote(block(zz, y, s), block(zz, y, s), gy_send.at[zz, s, e - 1],
                      gy_recv.at[zz, s, e - 1], dev(z, x, mod(y, e, ny), c))

    def y_recv(zz, s, e):
        view = block(zz, mod(y, ny - e, ny), s)
        return remote(view, view, gy_send.at[zz, s, e - 1], gy_recv.at[zz, s, e - 1],
                      dev(z, x, mod(y, e, ny), c))

    for s in range(GATHER_CUTS):
        pl.when(z + 1 < nz)(lambda s=s: go_right(z, s).start())
        pl.when(z >= 1)(lambda s=s: go_left(z, s).start())
        for e in range(1, ny):
            go_y(z, s, e).start()
    relay_own((2,))
    for j in range(1, min(EARLY_GROUPS, p.nj)):
        relay((0, 1), j)
    for dist in range(1, nz):
        for s in range(GATHER_CUTS):

            @pl.when(z - dist >= 0)
            def _(dist=dist, s=s):
                go_right(z - dist, s).wait_recv()
                pl.when(z + 1 < nz)(lambda: go_right(z - dist, s).start())
                for e in range(1, ny):
                    go_y(z - dist, s, e).start()

            @pl.when(z + dist < nz)
            def _(dist=dist, s=s):
                go_left(z + dist, s).wait_recv()
                pl.when(z >= 1)(lambda: go_left(z + dist, s).start())
                for e in range(1, ny):
                    go_y(z + dist, s, e).start()

    for j in range(min(EARLY_GROUPS, p.nj), p.nj):
        send_group((0, 1), j)
    for j in range(p.nj):
        send_group((2,), j)
    for j in range(min(EARLY_GROUPS, p.nj)):
        settle((0, 1), j)
    if p.nj > EARLY_GROUPS:
        relay((0, 1), EARLY_GROUPS)
    for zz in range(nz):
        for s in range(GATHER_CUTS):
            for e in range(1, ny):
                y_recv(zz, s, e).wait_recv()
    for s in range(GATHER_CUTS):

        def sent(zz, s=s):
            pl.when((z + 1 < nz) & (zz <= z))(lambda: go_right(zz, s).wait_send())
            pl.when((z >= 1) & (zz >= z))(lambda: go_left(zz, s).wait_send())
            for e in range(1, ny):
                go_y(zz, s, e).wait_send()

        for zz in range(nz):
            sent(zz)

    trows = p.ny * p.own

    def load_slab(m, j):
        return [
            pltpu.make_async_copy(
                mats[m][1].at[s, jrows(j), :],
                slab.at[m, pl.ds(s * LANES, LANES), :],
                local.at[m],
            )
            for s in range(p.sp)
        ]

    def whole_slab(m):
        return pltpu.make_async_copy(slab.at[m], slab.at[m], local.at[m])

    for j in range(p.nj):
        if j >= EARLY_GROUPS:
            if j + 1 < p.nj:
                relay((0, 1), j + 1)
            settle((0, 1), j)
        for m in range(2):
            for copy in load_slab(m, j):
                copy.start()
        for m in range(2):
            whole_slab(m).wait()

        @pl.loop(0, nz)
        def _(zz, j=j):
            lhs = jnp.concatenate(
                [
                    tokens[zz, :, :, s * p.rows + j * LANES : s * p.rows + (j + 1) * LANES].reshape(
                        trows, LANES
                    )
                    for s in range(p.sp)
                ],
                axis=1,
            )
            for m in range(2):
                more = dotf(lhs, slab[m])
                if j == 0:
                    acc[zz, m] = more
                else:
                    acc[zz, m] += more

    relay((2,), 0)

    @pl.loop(0, nz)
    def _(zz):
        hidden = jax.nn.silu(acc[zz, 0]) * acc[zz, 1]
        if any(p.dup):
            seen_col = lax.broadcasted_iota(jnp.int32, (1, p.hid), 1)
            for i in range(p.zc):
                if p.dup[i]:
                    drop = (seen_col < p.dup[i]) & (lax.rem(z, p.zc) == i)
                    hidden = jnp.where(drop, 0.0, hidden)
        tokens[zz, :, :, : p.hid] = hidden.astype(BF16).reshape(ny, p.own, p.hid)

    def ry(n, e):
        return remote(
            parts.at[n, :, mod(y, e, ny)], yb.at[n, e - 1], ry_send.at[n, e - 1],
            ry_recv.at[n, e - 1], dev(z, x, mod(y, e, ny), c),
        )

    def rz_right(n, o):
        return remote(parts.at[n, o, y], lb.at[n, o - 1], rr_send.at[n, o], rl_recv.at[n, o],
                      dev(z + 1, x, y, c))

    def rz_left(n, o):
        return remote(parts.at[n, o, y], rb.at[n, o], rl_send.at[n, o], rr_recv.at[n, o],
                      dev(z - 1, x, y, c))

    for yy in range(ny):
        at_peer(yy).wait_send()
    for e in range(1, ny):
        at_y(e).wait_send()

    def add_stream(n, more):
        j, half = n // p.halves, lax.rem(n, p.halves)
        for q in range(p.sph):
            at = pl.multiple_of((half * p.sph + q) * p.rows + j * LANES, LANES)
            stream[:, pl.ds(at, LANES)] += 0.5 * more[:, q * LANES : (q + 1) * LANES]

    def load_down(n):
        j, half = n // p.halves, lax.rem(n, p.halves)
        return [
            pltpu.make_async_copy(
                down_b.at[half * p.sph + q, jrows(j), :],
                slab.at[0, pl.ds(q * LANES, LANES), :],
                local.at[0],
            )
            for q in range(p.sph)
        ]

    def step(i, _):
        @pl.when(i < p.ns)
        def _():
            j = i // p.halves

            @pl.when(lax.rem(i, p.halves) == 0)
            def _():
                settle((2,), j)

            for copy in load_down(i):
                copy.start()
            view = slab.at[0, pl.ds(0, p.sph * LANES), :]
            pltpu.make_async_copy(view, view, local.at[0]).wait()

            @pl.loop(0, nz)
            def _(zz):
                hid = tokens[zz, :, :, : p.hid].reshape(trows, p.hid)
                terms = dotf(hid, slab[0, : p.sph * LANES, :], (((1,), (1,)), ((), ())))
                parts[i, zz] = terms.astype(BF16).reshape(ny, p.own, p.cw)

            for e in range(1, ny):
                ry(i, e).start()

            @pl.when((lax.rem(i, p.halves) == 0) & (j + 1 < p.nj))
            def _():
                relay((2,), j + 1)

        @pl.when((i >= 1) & (i <= p.ns))
        def _():
            n = i - 1
            for e in range(1, ny):
                ry(n, e).wait_recv()

            @pl.loop(0, nz)
            def _(o):
                total = parts[n, o, y].astype(F32)
                for e in range(1, ny):
                    total += yb[n, e - 1, o].astype(F32)
                parts[n, o, y] = total.astype(BF16)
                pl.when(o == z)(lambda: add_stream(n, total))

        right = i - 1 - z

        @pl.when((right >= 0) & (right < p.ns))
        def _():
            for o in range(nz - 1, 0, -1):

                @pl.when((o >= z) & (z > 0))
                def _(o=o):
                    rz_right(right, o).wait_recv()

                @pl.when((o > z) & (z > 0))
                def _(o=o):
                    parts[right, o, y] = (
                        parts[right, o, y].astype(F32) + lb[right, o - 1].astype(F32)
                    ).astype(BF16)

                pl.when(o > z)(lambda o=o: rz_right(right, o).start())
                pl.when(o == z)(lambda o=o: add_stream(right, lb[right, o - 1].astype(F32)))

        left = i - 1 - (nz - 1 - z)

        @pl.when((left >= 0) & (left < p.ns))
        def _():
            for o in range(nz - 1):

                @pl.when((o <= z) & (z < nz - 1))
                def _(o=o):
                    rz_left(left, o).wait_recv()

                @pl.when((o < z) & (z < nz - 1))
                def _(o=o):
                    parts[left, o, y] = (
                        parts[left, o, y].astype(F32) + rb[left, o].astype(F32)
                    ).astype(BF16)

                pl.when(o < z)(lambda o=o: rz_left(left, o).start())
                pl.when(o == z)(lambda o=o: add_stream(left, rb[left, o].astype(F32)))

        return 0

    lax.fori_loop(0, p.ns + nz, step, 0)
    out[...] = stream[...].astype(BF16)

    for e in range(1, nx):
        state_x(e).wait_send()
    for dist in range(1, nz):
        pl.when(z + dist < nz)(lambda dist=dist: state_z(dist).wait_send())

    @pl.loop(0, p.nj)
    def _(j):
        for m in range(3):
            for i in range(p.zc):
                first_hop(m, j, i).wait_send()

            @pl.when(duty)
            def _(m=m):
                for zz in range(nz):
                    for e in range(1, nx):
                        across(m, j, zz, e).wait_send()
                peer_all(m, j).wait_send()

    @pl.loop(0, p.ns)
    def _(n):
        for e in range(1, ny):
            ry(n, e).wait_send()
        for o in range(nz):
            if o:
                pl.when(o > z)(lambda o=o: rz_right(n, o).wait_send())
            if o < nz - 1:
                pl.when(o < z)(lambda o=o: rz_left(n, o).wait_send())


def solution(mesh):
    def per_device(*args):
        (residual, queries, keys, values, out_gate, in_gate, forget, extra, head_gain, out_w,
         ff_gain, gate_w, up_w, down_w) = args
        p = Plan(
            dict(mesh.shape),
            {
                "residual": residual.shape, "queries": queries.shape, "values": values.shape,
                "gates": in_gate.shape, "gate": gate_w.shape,
            },
        )
        vmem = pl.BlockSpec(memory_space=pltpu.VMEM)
        hbm = pl.BlockSpec(memory_space=pl.ANY)
        dma = pltpu.SemaphoreType.DMA
        held = jax.ShapeDtypeStruct((p.sp, p.rows, p.hid), BF16)
        nj, nz, nx, ny, ns = p.nj, p.nz, p.nx, p.ny, p.ns
        cols_used = p.d // p.cw
        cols8 = -(-2 * p.heads // 8) * 8
        scratch = [
            pltpu.VMEM((p.tok, cols8), F32),
            pltpu.VMEM((p.tok, p.vw), BF16),
            pltpu.VMEM((nx, p.state_rows, LANES), F32),
            pltpu.VMEM((nz, p.state_rows, LANES), F32),
            pltpu.VMEM((p.state_rows, LANES), F32),
            pltpu.VMEM((nz, ny, p.own, p.d), BF16),
            pltpu.VMEM((nz, 2, ny * p.own, p.hid), F32),
            pltpu.VMEM((2, p.sp * LANES, p.hid), BF16),
            pltpu.VMEM((ns, nz, ny, p.own, p.cw), BF16),
            pltpu.VMEM((ns, ny - 1, nz, p.own, p.cw), BF16),
            pltpu.VMEM((ns, nz - 1, p.own, p.cw), BF16),
            pltpu.VMEM((ns, nz - 1, p.own, p.cw), BF16),
            pltpu.VMEM((p.own, p.d), F32),
            pltpu.VMEM((cols_used, ny, p.own, p.cw), BF16),
            pltpu.VMEM((cols_used, ny - 1, p.own, p.cw), BF16),
            pltpu.VMEM((p.own, p.d), BF16),
            dma((3, nj, p.zc)), dma((3, nj, nz)),
            dma((3, nj, nz, nx - 1)), dma((3, nj, nz, nx - 1)),
            dma((3, nj)), dma((3, nj)),
            dma((nx - 1,)), dma((nx - 1,)),
            dma((nz - 1,)), dma((nz,)),
            dma((ny,)), dma((ny,)), dma((ny - 1,)), dma((ny - 1,)),
            dma((nz, GATHER_CUTS)), dma((nz, GATHER_CUTS)), dma((nz, GATHER_CUTS)),
            dma((nz, GATHER_CUTS, ny - 1)), dma((nz, GATHER_CUTS, ny - 1)),
            dma((ns, ny - 1)), dma((ns, ny - 1)),
            dma((ns, nz)), dma((ns, nz)), dma((ns, nz)), dma((ns, nz)),
            dma((3,)),
        ]
        result = pl.pallas_call(
            functools.partial(layer, p),
            out_shape=(
                jax.ShapeDtypeStruct((p.own, p.d), BF16), held, held, held,
            ),
            in_specs=[hbm] + [vmem] * 8 + [hbm, vmem] + [hbm] * 3,
            out_specs=(vmem, hbm, hbm, hbm),
            scratch_shapes=scratch,
            compiler_params=pltpu.CompilerParams(
                collective_id=0, has_side_effects=True, vmem_limit_bytes=67043328
            ),
            name="layer",
        )(
            residual, queries, keys, values, out_gate, in_gate, forget, extra,
            head_gain.reshape(1, -1), out_w, ff_gain.reshape(1, -1), gate_w, up_w, down_w,
        )
        return result[0]

    in_specs = (
        P("sp", None), P("sp", "tp"), P("sp", "tp"), P("sp", "tp"), P("sp", "tp"),
        P("tp", "sp"), P("tp", "sp"), P("tp", "sp"), P("tp"), P("tp", None), P(),
        P("sp", "tp"), P("sp", "tp"), P("sp", "tp"),
    )
    return jax.shard_map(
        per_device, mesh=mesh, in_specs=in_specs, out_specs=P(("sp", "tp"), None), check_vma=False
    )
```

```python
import functools
import jax
import jax.numpy as jnp
from jax import lax
from jax.experimental import pallas as pl
from jax.experimental.pallas import tpu as pltpu
from jax.sharding import PartitionSpec as P

MESH = pl.DeviceIdType.MESH
F32 = jnp.float32
BF16 = jnp.bfloat16
LANES = 128
QUERY_ROWS = 256
TOKEN_ROWS = 256
GATHER_CUTS = 2
EARLY_GROUPS = 2


class Plan:
    def __init__(self, mesh_shape, shapes):
        self.sp, self.tp = mesh_shape["sp"], mesh_shape["tp"]
        self.nz = next(n for n in range(1, self.sp + 1) if self.sp % n == 0 and n * n >= self.sp)
        self.nx = self.sp // self.nz
        self.nc = 2
        self.ny = self.tp // self.nc
        self.tok, self.d = shapes["residual"]
        self.own = self.tok // self.tp
        self.heads = shapes["gates"][0]
        self.qk = shapes["queries"][1] // self.heads
        self.vd = shapes["values"][1] // self.heads
        self.per = LANES // self.qk
        self.pairs = self.heads // self.per
        self.vw = shapes["values"][1]
        self.rows, self.ff = shapes["gate"]
        self.zc = self.nz // self.nc
        tiles = self.ff // LANES
        wide = -(-tiles // self.zc)
        starts = [min(i * wide, tiles - wide) for i in range(self.zc)]
        self.start = [s * LANES for s in starts]
        self.dup = [(i * wide - s) * LANES for i, s in enumerate(starts)]
        self.hid = wide * LANES
        self.nj = self.rows // LANES
        self.halves = 2
        self.sph = self.sp // self.halves
        self.cw = self.sph * LANES
        self.ns = self.nj * self.halves
        self.toks = self.nz * self.ny * self.own
        self.state_rows = self.pairs * LANES + -(-(self.pairs + 2 * self.heads) // 8) * 8
        self.wc = next(
            n for n in range(self.hid // LANES * LANES, 0, -LANES) if self.d % n == 0
        )
        self.cc = min(self.cw, self.wc)


def dotf(a, b, dims=(((1,), (0,)), ((), ())), precision=None):
    return lax.dot_general(a, b, dims, preferred_element_type=F32, precision=precision)


def split(a):
    high = a.astype(BF16)
    return high, (a - high.astype(F32)).astype(BF16)


def layer(p, *refs):
    (
        residual, queries, keys, values, out_gate, in_gate, forget, extra, head_gain, out_w,
        ff_gain, gate_w, up_w, down_w,
        out, gate_b, up_b, down_b,
        col, gated, xs, zs, carry, tokens, acc, slab, parts, yb, lb, rb, stream, cr, yr, res,
        s1_send, s1_recv, xf_send, xf_recv, pf_send, pf_recv,
        stx_send, stx_recv, stz_send, stz_recv, at_send, at_recv, ay_send, ay_recv,
        gz_right, gz_left, gz_recv, gy_send, gy_recv,
        ry_send, ry_recv, rr_send, rl_send, rl_recv, rr_recv, local,
    ) = refs
    nz, nx, ny, nc = p.nz, p.nx, p.ny, p.nc
    sp_i, tp_i = lax.axis_index("sp"), lax.axis_index("tp")
    z, x = sp_i // nx, lax.rem(sp_i, nx)
    y, c = tp_i // nc, lax.rem(tp_i, nc)
    other = 1 - c
    duty = c == 1 - z // p.zc

    def dev(z_, x_, y_, c_):
        return (z_ * nx + x_, y_ * nc + c_)

    def mod(a, e, n):
        return lax.rem(a + e, n)

    def remote(src, dst, send, recv, device):
        return pltpu.make_async_remote_copy(
            src_ref=src, dst_ref=dst, send_sem=send, recv_sem=recv,
            device_id=device, device_id_type=MESH,
        )

    barrier = pltpu.get_barrier_semaphore()
    friends = [dev(mod(z, e, nz), x, y, c) for e in range(1, nz)]
    friends += [dev(z, mod(x, e, nx), y, c) for e in range(1, nx)]
    friends += [dev(z, x, mod(y, e, ny), c) for e in range(1, ny)]
    friends += [dev(mod(z, e, nz), x, y, other) for e in range(nz)]
    for friend in friends:
        pl.semaphore_signal(barrier, inc=1, device_id=friend, device_id_type=MESH)
    pl.semaphore_wait(barrier, len(friends))

    mats = ((gate_w, gate_b), (up_w, up_b), (down_w, down_b))

    def jrows(j):
        return pl.ds(pl.multiple_of(j * LANES, LANES), LANES)

    def first_hop(m, j, i):
        src, dst = mats[m]
        return remote(
            src.at[jrows(j), pl.ds(p.start[i], p.hid)],
            dst.at[sp_i, jrows(j), :],
            s1_send.at[m, j, i], s1_recv.at[m, j, z],
            dev(c * p.zc + i, x, y, other),
        )

    def first_recv(m, j, zs_):
        src, dst = mats[m]
        view = dst.at[zs_ * nx + x, jrows(j), :]
        return remote(view, view, s1_send.at[m, j, 0], s1_recv.at[m, j, zs_], dev(z, x, y, other))

    def across(m, j, zs_, e):
        view = mats[m][1].at[zs_ * nx + x, jrows(j), :]
        return remote(
            view, view, xf_send.at[m, j, zs_, e - 1], xf_recv.at[m, j, zs_, e - 1],
            dev(z, mod(x, e, nx), y, c),
        )

    def across_recv(m, j, zs_, e):
        view = mats[m][1].at[zs_ * nx + mod(x, nx - e, nx), jrows(j), :]
        return remote(
            view, view, xf_send.at[m, j, zs_, e - 1], xf_recv.at[m, j, zs_, e - 1],
            dev(z, mod(x, e, nx), y, c),
        )

    def to_peer(m, j, sp_):
        view = mats[m][1].at[sp_, jrows(j), :]
        return remote(view, view, pf_send.at[m, j], pf_recv.at[m, j], dev(z, x, y, other))

    def peer_all(m, j):
        view = mats[m][1].at[:, jrows(j), :]
        return remote(view, view, pf_send.at[m, j], pf_recv.at[m, j], dev(z, x, y, other))

    def send_group(ms, j):
        for i in range(p.zc):

            @pl.when(c * p.zc + i != z)
            def _(i=i):
                for m in ms:
                    first_hop(m, j, i).start()

    def send_own():
        for i in range(p.zc):

            @pl.when(c * p.zc + i == z)
            def _(i=i):
                for m in range(3):
                    for j in range(p.nj):
                        first_hop(m, j, i).start()

    def each_other(fn):
        for dist in range(1, nz):
            pl.when(z - dist >= 0)(functools.partial(fn, z - dist))
            pl.when(z + dist < nz)(functools.partial(fn, z + dist))

    def each_z(fn):
        fn(z)
        each_other(fn)

    def pass_on(ms, j, zs_):
        for m in ms:
            first_recv(m, j, zs_).wait_recv()
            for e in range(1, nx):
                across(m, j, zs_, e).start()
            to_peer(m, j, zs_ * nx + x).start()

    def relay(ms, j):
        @pl.when(duty)
        def _():
            each_other(functools.partial(pass_on, ms, j))

    def relay_own(ms):
        @pl.when(duty)
        def _():
            for j in range(p.nj):
                pass_on(ms, j, z)

    def settle(ms, j):
        @pl.when(duty)
        def _():
            def one(zs_):
                for m in ms:
                    for e in range(1, nx):
                        across_recv(m, j, zs_, e).wait_recv()
                        to_peer(m, j, zs_ * nx + mod(x, nx - e, nx)).start()

            each_z(one)

        @pl.when(jnp.logical_not(duty))
        def _():
            for m in ms:
                peer_all(m, j).wait_recv()

    send_group((0,), 0)
    send_own()
    fetch_res = pltpu.make_async_copy(
        residual.at[pl.ds(pl.multiple_of(tp_i * p.own, p.own), p.own), :], res, local.at[2]
    )
    fetch_res.start()

    heads, per, pairs, tok = p.heads, p.per, p.pairs, p.tok
    fg = forget[...]
    lf = jnp.minimum(fg, 0.0) - jnp.log1p(jnp.exp(-jnp.abs(fg))) + extra[...]
    upper = (
        lax.broadcasted_iota(jnp.int32, (tok, tok), 0)
        <= lax.broadcasted_iota(jnp.int32, (tok, tok), 1)
    ).astype(F32)
    pad = jnp.zeros((-heads % 8, tok), F32)
    lf8 = jnp.concatenate([lf, pad], axis=0) if pad.shape[0] else lf
    cum_row = dotf(lf8, upper, precision=lax.Precision.HIGHEST)[:heads]
    ig = in_gate[...]
    pad = jnp.zeros((-2 * heads % 8, tok), F32)
    both = [cum_row, ig] + ([pad] if pad.shape[0] else [])
    col[...] = jnp.concatenate(both, axis=0).T
    bias_row = ig - cum_row
    base = pairs * LANES
    lane = lax.broadcasted_iota(jnp.int32, (1, LANES), 1) // p.qk
    subl = lax.broadcasted_iota(jnp.int32, (LANES, 1), 0) // p.qk

    def head_lanes(ref, h):
        pair = ref[:, h // per * LANES : (h // per + 1) * LANES]
        return jnp.where(lane == h % per, pair, jnp.zeros_like(pair))

    for pr in range(pairs):
        state = jnp.zeros((LANES, LANES), F32)
        norm = jnp.zeros((1, LANES), F32)
        for h in range(pr * per, (pr + 1) * per):
            total = cum_row[h : h + 1, tok - 1 : tok]
            log_w = total - col[:, h : h + 1] + col[:, heads + h : heads + h + 1]
            peak = jnp.max(log_w, axis=0, keepdims=True)
            weight = jnp.exp(log_w - peak)
            k_h = head_lanes(keys, h)
            high, low = split(values[:, h * p.vd : (h + 1) * p.vd].astype(F32) * weight)
            over = (((0,), (0,)), ((), ()))
            state += dotf(k_h, high, over) + dotf(k_h, low, over)
            norm += jnp.sum(k_h.astype(F32) * weight, axis=0, keepdims=True)
            row = base + pairs + h
            xs[x, row : row + 1, :] = jnp.broadcast_to(total, (1, LANES))
            row = base + pairs + heads + h
            xs[x, row : row + 1, :] = jnp.broadcast_to(peak, (1, LANES))
        xs[x, pr * LANES : (pr + 1) * LANES, :] = state
        xs[x, base + pr : base + pr + 1, :] = norm
    spare = p.state_rows - base - pairs - 2 * heads
    if spare:
        xs[x, p.state_rows - spare :, :] = jnp.zeros((spare, LANES), F32)

    def state_x(e):
        return remote(
            xs.at[x], xs.at[x], stx_send.at[e - 1], stx_recv.at[e - 1],
            dev(z, mod(x, e, nx), y, c),
        )

    def state_x_recv(e):
        view = xs.at[mod(x, nx - e, nx)]
        return remote(view, view, stx_send.at[e - 1], stx_recv.at[e - 1], dev(z, mod(x, e, nx), y, c))

    for e in range(1, nx):
        state_x(e).start()

    def join(target, later):
        lo = base + pairs
        tot_e, tot_l = target[lo : lo + heads, :], later[lo : lo + heads, :]
        pk_e = target[lo + heads : lo + 2 * heads, :]
        pk_l = later[lo + heads : lo + 2 * heads, :]
        pk = jnp.maximum(tot_l + pk_e, pk_l)
        w_e, w_l = jnp.exp(tot_l + pk_e - pk), jnp.exp(pk_l - pk)
        for pr in range(pairs):
            hs = [pr * per + i for i in range(per)]
            e_col = jnp.zeros((LANES, LANES), F32)
            l_col = jnp.zeros((LANES, LANES), F32)
            e_row = jnp.zeros((1, LANES), F32)
            l_row = jnp.zeros((1, LANES), F32)
            for i, h in enumerate(hs):
                e_col = jnp.where(subl == i, w_e[h : h + 1, :], e_col)
                l_col = jnp.where(subl == i, w_l[h : h + 1, :], l_col)
                e_row = jnp.where(lane == i, w_e[h : h + 1, :], e_row)
                l_row = jnp.where(lane == i, w_l[h : h + 1, :], l_row)
            blk = slice(pr * LANES, (pr + 1) * LANES)
            target[blk, :] = e_col * target[blk, :] + l_col * later[blk, :]
            row = slice(base + pr, base + pr + 1)
            target[row, :] = e_row * target[row, :] + l_row * later[row, :]
        target[lo : lo + heads, :] = tot_e + tot_l
        target[lo + heads : lo + 2 * heads, :] = pk

    def reset(target):
        target[...] = jnp.zeros((p.state_rows, LANES), F32)
        lo = base + pairs + heads
        target[lo : lo + heads, :] = jnp.full((heads, LANES), -1e30, F32)

    for e in range(1, nx):
        state_x_recv(e).wait_recv()
    mine = zs.at[z]
    reset(mine)
    for i in range(nx):
        join(mine, xs.at[i])

    def state_z(dist):
        return remote(
            zs.at[z], zs.at[z], stz_send.at[dist - 1], stz_recv.at[z],
            dev(lax.rem(z + dist, nz), x, y, c),
        )

    for dist in range(1, nz):
        pl.when(z + dist < nz)(lambda dist=dist: state_z(dist).start())
    send_group((1,), 0)
    for j in range(1, min(EARLY_GROUPS, p.nj)):
        send_group((0, 1), j)
    relay_own((0, 1))

    reset(carry)
    for i in range(nz - 1):

        @pl.when(i < z)
        def _(i=i):
            remote(zs.at[i], zs.at[i], stz_send.at[0], stz_recv.at[i], dev(z, x, y, other)).wait_recv()
            join(carry, zs.at[i])

    for i in range(nx - 1):
        pl.when(i < x)(lambda i=i: join(carry, xs.at[i]))

    lo = base + pairs
    total_in = carry[lo : lo + heads, :]
    peak_raw = carry[lo + heads : lo + 2 * heads, :]
    peak_all = jnp.maximum(peak_raw, total_in)
    scale_all = jnp.exp(peak_raw - peak_all)
    unit = p.qk ** (-0.5)
    qrows = min(QUERY_ROWS, tok)
    for h in range(heads):
        pr = h // per
        peak_in = peak_all[h : h + 1, 0:1]
        scale = scale_all[h : h + 1, :]
        st_high, st_low = split(carry[pr * LANES : (pr + 1) * LANES, :] * scale)
        norm_in = carry[base + pr : base + pr + 1, :] * scale
        k2 = keys[:, pr * LANES : (pr + 1) * LANES]
        v_h = values[:, h * p.vd : (h + 1) * p.vd]
        for r0 in range(0, tok, qrows):
            r1 = r0 + qrows
            q2 = queries[r0:r1, pr * LANES : (pr + 1) * LANES]
            q_h = jnp.where(lane == h % per, q2, jnp.zeros_like(q2))
            cum_c = col[r0:r1, h : h + 1]
            seen = (
                lax.broadcasted_iota(jnp.int32, (qrows, r1), 0) + r0
                >= lax.broadcasted_iota(jnp.int32, (qrows, r1), 1)
            )
            logs = jnp.where(seen, bias_row[h : h + 1, :r1], -jnp.inf) + cum_c
            inter = cum_c + peak_in
            peak_row = jnp.maximum(inter, jnp.max(logs, axis=1, keepdims=True))
            dots = dotf(q_h, k2[:r1], (((1,), (1,)), ((), ()))) * unit
            probs = dots * jnp.exp(logs - peak_row)
            inter_scale = jnp.exp(inter - peak_row) * unit
            high, low = split(probs)
            numer = dotf(high, v_h[:r1]) + dotf(low, v_h[:r1])
            numer += inter_scale * (dotf(q_h, st_high) + dotf(q_h, st_low))
            denom = jnp.sum(probs, axis=1, keepdims=True) + inter_scale * jnp.sum(
                q_h.astype(F32) * norm_in, axis=1, keepdims=True
            )
            cell = numer / jnp.maximum(jnp.abs(denom), jnp.exp(-peak_row))
            square = jnp.mean(cell * cell, axis=1, keepdims=True)
            span = slice(h * p.vd, (h + 1) * p.vd)
            gain = head_gain[:, span].astype(F32)
            gates = jax.nn.sigmoid(out_gate[r0:r1, span].astype(F32))
            gated[r0:r1, span] = (cell * lax.rsqrt(square + 1e-06) * gain * gates).astype(BF16)

    pieces = p.d // p.wc

    def fetch_w(n):
        return pltpu.make_async_copy(
            out_w.at[:, pl.ds(n * p.wc, p.wc)],
            slab.at[n % 2, pl.ds(0, p.vw), pl.ds(0, p.wc)],
            local.at[n % 2],
        )

    fetch_w(0).start()
    for n in range(pieces):
        if n + 1 < pieces:
            fetch_w(n + 1).start()
        fetch_w(n).wait()
        for c0 in range(0, p.wc, p.cc):
            g0 = n * p.wc + c0
            w = slab[n % 2, : p.vw, c0 : c0 + p.cc]
            res_ = dotf(gated[...], w).astype(BF16)
            for b in range(p.tp):
                parts[g0 // p.cw, b // ny, b % ny, :, g0 % p.cw : g0 % p.cw + p.cc] = res_[
                    b * p.own : (b + 1) * p.own
                ]

    cols_used = p.d // p.cw

    def at_peer(yy):
        b = yy * nc + other
        return remote(
            parts.at[pl.ds(0, cols_used), b // ny, lax.rem(b, ny)],
            cr.at[:, yy], at_send.at[yy], at_recv.at[yy], dev(z, x, y, other),
        )

    for yy in range(ny):
        at_peer(yy).start()

    def at_y(e):
        b = mod(y, e, ny) * nc + c
        return remote(
            parts.at[pl.ds(0, cols_used), b // ny, lax.rem(b, ny)],
            yr.at[:, e - 1], ay_send.at[e - 1], ay_recv.at[e - 1], dev(z, x, mod(y, e, ny), c),
        )

    for yy in range(ny):
        at_peer(yy).wait_recv()
    for e in range(1, ny):
        to = mod(y, e, ny)
        b = to * nc + c
        for n in range(cols_used):
            parts[n, b // ny, lax.rem(b, ny)] = (
                parts[n, b // ny, lax.rem(b, ny)].astype(F32) + cr[n, to].astype(F32)
            ).astype(BF16)
        at_y(e).start()
    fetch_res.wait()
    b = y * nc + c
    for n in range(cols_used):
        cols = slice(n * p.cw, (n + 1) * p.cw)
        stream[:, cols] = (
            res[:, cols].astype(F32)
            + parts[n, b // ny, lax.rem(b, ny)].astype(F32) + cr[n, y].astype(F32)
        )
    relay((0, 1), 0)
    for e in range(1, ny):
        at_y(e).wait_recv()
        for n in range(cols_used):
            cols = slice(n * p.cw, (n + 1) * p.cw)
            stream[:, cols] += yr[n, e - 1].astype(F32)
    cut = p.own // GATHER_CUTS
    for s in range(GATHER_CUTS):
        rows = slice(s * cut, (s + 1) * cut)
        part = stream[rows, :]
        square = jnp.mean(part * part, axis=1, keepdims=True)
        tokens[z, y, rows, :] = (
            part * lax.rsqrt(square + 1e-06) * ff_gain[...].astype(F32)
        ).astype(BF16)

    def block(zz, yy, s):
        return tokens.at[zz, yy, pl.ds(s * cut, cut), :]

    def go_right(zz, s):
        return remote(block(zz, y, s), block(zz, y, s), gz_right.at[zz, s], gz_recv.at[zz, s],
                      dev(z + 1, x, y, c))

    def go_left(zz, s):
        return remote(block(zz, y, s), block(zz, y, s), gz_left.at[zz, s], gz_recv.at[zz, s],
                      dev(z - 1, x, y, c))

    def go_y(zz, s, e):
        return remote(block(zz, y, s), block(zz, y, s), gy_send.at[zz, s, e - 1],
                      gy_recv.at[zz, s, e - 1], dev(z, x, mod(y, e, ny), c))

    def y_recv(zz, s, e):
        view = block(zz, mod(y, ny - e, ny), s)
        return remote(view, view, gy_send.at[zz, s, e - 1], gy_recv.at[zz, s, e - 1],
                      dev(z, x, mod(y, e, ny), c))

    for s in range(GATHER_CUTS):
        pl.when(z + 1 < nz)(lambda s=s: go_right(z, s).start())
        pl.when(z >= 1)(lambda s=s: go_left(z, s).start())
        for e in range(1, ny):
            go_y(z, s, e).start()
    relay_own((2,))
    for j in range(1, min(EARLY_GROUPS, p.nj)):
        relay((0, 1), j)
    for dist in range(1, nz):
        for s in range(GATHER_CUTS):

            @pl.when(z - dist >= 0)
            def _(dist=dist, s=s):
                go_right(z - dist, s).wait_recv()
                pl.when(z + 1 < nz)(lambda: go_right(z - dist, s).start())
                for e in range(1, ny):
                    go_y(z - dist, s, e).start()

            @pl.when(z + dist < nz)
            def _(dist=dist, s=s):
                go_left(z + dist, s).wait_recv()
                pl.when(z >= 1)(lambda: go_left(z + dist, s).start())
                for e in range(1, ny):
                    go_y(z + dist, s, e).start()

    for j in range(min(EARLY_GROUPS, p.nj), p.nj):
        send_group((0, 1), j)
    for j in range(p.nj):
        send_group((2,), j)
    for j in range(min(EARLY_GROUPS, p.nj)):
        settle((0, 1), j)
    if p.nj > EARLY_GROUPS:
        relay((0, 1), EARLY_GROUPS)
    for zz in range(nz):
        for s in range(GATHER_CUTS):
            for e in range(1, ny):
                y_recv(zz, s, e).wait_recv()
    for s in range(GATHER_CUTS):

        def sent(zz, s=s):
            pl.when((z + 1 < nz) & (zz <= z))(lambda: go_right(zz, s).wait_send())
            pl.when((z >= 1) & (zz >= z))(lambda: go_left(zz, s).wait_send())
            for e in range(1, ny):
                go_y(zz, s, e).wait_send()

        for zz in range(nz):
            sent(zz)

    trows = p.ny * p.own

    def load_slab(m, j):
        return [
            pltpu.make_async_copy(
                mats[m][1].at[s, jrows(j), :],
                slab.at[m, pl.ds(s * LANES, LANES), :],
                local.at[m],
            )
            for s in range(p.sp)
        ]

    def whole_slab(m):
        return pltpu.make_async_copy(slab.at[m], slab.at[m], local.at[m])

    for j in range(p.nj):
        if j >= EARLY_GROUPS:
            if j + 1 < p.nj:
                relay((0, 1), j + 1)
            else:
                relay((2,), 0)
            settle((0, 1), j)
        for m in range(2):
            for copy in load_slab(m, j):
                copy.start()
        for m in range(2):
            whole_slab(m).wait()

        @pl.loop(0, nz)
        def _(zz, j=j):
            lhs = jnp.concatenate(
                [
                    tokens[zz, :, :, s * p.rows + j * LANES : s * p.rows + (j + 1) * LANES].reshape(
                        trows, LANES
                    )
                    for s in range(p.sp)
                ],
                axis=1,
            )
            for m in range(2):
                more = dotf(lhs, slab[m])
                if j == 0:
                    acc[zz, m] = more
                else:
                    acc[zz, m] += more

    if p.nj <= EARLY_GROUPS:
        relay((2,), 0)
    if p.nj > 1:
        relay((2,), 1)

    @pl.loop(0, nz)
    def _(zz):
        hidden = jax.nn.silu(acc[zz, 0]) * acc[zz, 1]
        if any(p.dup):
            seen_col = lax.broadcasted_iota(jnp.int32, (1, p.hid), 1)
            for i in range(p.zc):
                if p.dup[i]:
                    drop = (seen_col < p.dup[i]) & (lax.rem(z, p.zc) == i)
                    hidden = jnp.where(drop, 0.0, hidden)
        tokens[zz, :, :, : p.hid] = hidden.astype(BF16).reshape(ny, p.own, p.hid)

    def ry(n, e):
        return remote(
            parts.at[n, :, mod(y, e, ny)], yb.at[n, e - 1], ry_send.at[n, e - 1],
            ry_recv.at[n, e - 1], dev(z, x, mod(y, e, ny), c),
        )

    def rz_right(n, o):
        return remote(parts.at[n, o, y], lb.at[n, o - 1], rr_send.at[n, o], rl_recv.at[n, o],
                      dev(z + 1, x, y, c))

    def rz_left(n, o):
        return remote(parts.at[n, o, y], rb.at[n, o], rl_send.at[n, o], rr_recv.at[n, o],
                      dev(z - 1, x, y, c))

    for yy in range(ny):
        at_peer(yy).wait_send()
    for e in range(1, ny):
        at_y(e).wait_send()

    def add_stream(n, more):
        j, half = n // p.halves, lax.rem(n, p.halves)
        for q in range(p.sph):
            at = pl.multiple_of((half * p.sph + q) * p.rows + j * LANES, LANES)
            stream[:, pl.ds(at, LANES)] += 0.5 * more[:, q * LANES : (q + 1) * LANES]

    def load_down(n):
        j, half = n // p.halves, lax.rem(n, p.halves)
        return [
            pltpu.make_async_copy(
                down_b.at[half * p.sph + q, jrows(j), :],
                slab.at[0, pl.ds(q * LANES, LANES), :],
                local.at[0],
            )
            for q in range(p.sph)
        ]

    def step(i, _):
        @pl.when(i < p.ns)
        def _():
            j = i // p.halves

            @pl.when(lax.rem(i, p.halves) == 0)
            def _():
                settle((2,), j)

            for copy in load_down(i):
                copy.start()
            view = slab.at[0, pl.ds(0, p.sph * LANES), :]
            pltpu.make_async_copy(view, view, local.at[0]).wait()

            @pl.loop(0, nz)
            def _(zz):
                hid = tokens[zz, :, :, : p.hid].reshape(trows, p.hid)
                terms = dotf(hid, slab[0, : p.sph * LANES, :], (((1,), (1,)), ((), ())))
                parts[i, zz] = terms.astype(BF16).reshape(ny, p.own, p.cw)

            for e in range(1, ny):
                ry(i, e).start()

            @pl.when((lax.rem(i, p.halves) == 0) & (j + 2 < p.nj))
            def _():
                relay((2,), j + 2)

        @pl.when((i >= 1) & (i <= p.ns))
        def _():
            n = i - 1
            for e in range(1, ny):
                ry(n, e).wait_recv()

            @pl.loop(0, nz)
            def _(o):
                total = parts[n, o, y].astype(F32)
                for e in range(1, ny):
                    total += yb[n, e - 1, o].astype(F32)
                parts[n, o, y] = total.astype(BF16)
                pl.when(o == z)(lambda: add_stream(n, total))

        right = i - 1 - z

        @pl.when((right >= 0) & (right < p.ns))
        def _():
            for o in range(nz - 1, 0, -1):

                @pl.when((o >= z) & (z > 0))
                def _(o=o):
                    rz_right(right, o).wait_recv()

                @pl.when((o > z) & (z > 0))
                def _(o=o):
                    parts[right, o, y] = (
                        parts[right, o, y].astype(F32) + lb[right, o - 1].astype(F32)
                    ).astype(BF16)

                pl.when(o > z)(lambda o=o: rz_right(right, o).start())
                pl.when(o == z)(lambda o=o: add_stream(right, lb[right, o - 1].astype(F32)))

        left = i - 1 - (nz - 1 - z)

        @pl.when((left >= 0) & (left < p.ns))
        def _():
            for o in range(nz - 1):

                @pl.when((o <= z) & (z < nz - 1))
                def _(o=o):
                    rz_left(left, o).wait_recv()

                @pl.when((o < z) & (z < nz - 1))
                def _(o=o):
                    parts[left, o, y] = (
                        parts[left, o, y].astype(F32) + rb[left, o].astype(F32)
                    ).astype(BF16)

                pl.when(o < z)(lambda o=o: rz_left(left, o).start())
                pl.when(o == z)(lambda o=o: add_stream(left, rb[left, o].astype(F32)))

        return 0

    lax.fori_loop(0, p.ns + nz, step, 0)
    out[...] = stream[...].astype(BF16)

    for e in range(1, nx):
        state_x(e).wait_send()
    for dist in range(1, nz):
        pl.when(z + dist < nz)(lambda dist=dist: state_z(dist).wait_send())

    @pl.loop(0, p.nj)
    def _(j):
        for m in range(3):
            for i in range(p.zc):
                first_hop(m, j, i).wait_send()

            @pl.when(duty)
            def _(m=m):
                for zz in range(nz):
                    for e in range(1, nx):
                        across(m, j, zz, e).wait_send()
                peer_all(m, j).wait_send()

    @pl.loop(0, p.ns)
    def _(n):
        for e in range(1, ny):
            ry(n, e).wait_send()
        for o in range(nz):
            if o:
                pl.when(o > z)(lambda o=o: rz_right(n, o).wait_send())
            if o < nz - 1:
                pl.when(o < z)(lambda o=o: rz_left(n, o).wait_send())


def solution(mesh):
    def per_device(*args):
        (residual, queries, keys, values, out_gate, in_gate, forget, extra, head_gain, out_w,
         ff_gain, gate_w, up_w, down_w) = args
        p = Plan(
            dict(mesh.shape),
            {
                "residual": residual.shape, "queries": queries.shape, "values": values.shape,
                "gates": in_gate.shape, "gate": gate_w.shape,
            },
        )
        vmem = pl.BlockSpec(memory_space=pltpu.VMEM)
        hbm = pl.BlockSpec(memory_space=pl.ANY)
        dma = pltpu.SemaphoreType.DMA
        held = jax.ShapeDtypeStruct((p.sp, p.rows, p.hid), BF16)
        nj, nz, nx, ny, ns = p.nj, p.nz, p.nx, p.ny, p.ns
        cols_used = p.d // p.cw
        cols8 = -(-2 * p.heads // 8) * 8
        scratch = [
            pltpu.VMEM((p.tok, cols8), F32),
            pltpu.VMEM((p.tok, p.vw), BF16),
            pltpu.VMEM((nx, p.state_rows, LANES), F32),
            pltpu.VMEM((nz, p.state_rows, LANES), F32),
            pltpu.VMEM((p.state_rows, LANES), F32),
            pltpu.VMEM((nz, ny, p.own, p.d), BF16),
            pltpu.VMEM((nz, 2, ny * p.own, p.hid), F32),
            pltpu.VMEM((2, p.sp * LANES, p.hid), BF16),
            pltpu.VMEM((ns, nz, ny, p.own, p.cw), BF16),
            pltpu.VMEM((ns, ny - 1, nz, p.own, p.cw), BF16),
            pltpu.VMEM((ns, nz - 1, p.own, p.cw), BF16),
            pltpu.VMEM((ns, nz - 1, p.own, p.cw), BF16),
            pltpu.VMEM((p.own, p.d), F32),
            pltpu.VMEM((cols_used, ny, p.own, p.cw), BF16),
            pltpu.VMEM((cols_used, ny - 1, p.own, p.cw), BF16),
            pltpu.VMEM((p.own, p.d), BF16),
            dma((3, nj, p.zc)), dma((3, nj, nz)),
            dma((3, nj, nz, nx - 1)), dma((3, nj, nz, nx - 1)),
            dma((3, nj)), dma((3, nj)),
            dma((nx - 1,)), dma((nx - 1,)),
            dma((nz - 1,)), dma((nz,)),
            dma((ny,)), dma((ny,)), dma((ny - 1,)), dma((ny - 1,)),
            dma((nz, GATHER_CUTS)), dma((nz, GATHER_CUTS)), dma((nz, GATHER_CUTS)),
            dma((nz, GATHER_CUTS, ny - 1)), dma((nz, GATHER_CUTS, ny - 1)),
            dma((ns, ny - 1)), dma((ns, ny - 1)),
            dma((ns, nz)), dma((ns, nz)), dma((ns, nz)), dma((ns, nz)),
            dma((3,)),
        ]
        result = pl.pallas_call(
            functools.partial(layer, p),
            out_shape=(
                jax.ShapeDtypeStruct((p.own, p.d), BF16), held, held, held,
            ),
            in_specs=[hbm] + [vmem] * 8 + [hbm, vmem] + [hbm] * 3,
            out_specs=(vmem, hbm, hbm, hbm),
            scratch_shapes=scratch,
            compiler_params=pltpu.CompilerParams(
                collective_id=0, has_side_effects=True, vmem_limit_bytes=67043328
            ),
            name="layer",
        )(
            residual, queries, keys, values, out_gate, in_gate, forget, extra,
            head_gain.reshape(1, -1), out_w, ff_gain.reshape(1, -1), gate_w, up_w, down_w,
        )
        return result[0]

    in_specs = (
        P("sp", None), P("sp", "tp"), P("sp", "tp"), P("sp", "tp"), P("sp", "tp"),
        P("tp", "sp"), P("tp", "sp"), P("tp", "sp"), P("tp"), P("tp", None), P(),
        P("sp", "tp"), P("sp", "tp"), P("sp", "tp"),
    )
    return jax.shard_map(
        per_device, mesh=mesh, in_specs=in_specs, out_specs=P(("sp", "tp"), None), check_vma=False
    )
```

```python
import functools
import jax
import jax.numpy as jnp
from jax import lax
from jax.experimental import pallas as pl
from jax.experimental.pallas import tpu as pltpu
from jax.sharding import PartitionSpec as P

MESH = pl.DeviceIdType.MESH
F32 = jnp.float32
BF16 = jnp.bfloat16
LANES = 128
QUERY_ROWS = 256
TOKEN_ROWS = 256
GATHER_CUTS = 2
EARLY_GROUPS = 2


class Plan:
    def __init__(self, mesh_shape, shapes):
        self.sp, self.tp = mesh_shape["sp"], mesh_shape["tp"]
        self.nz = next(n for n in range(1, self.sp + 1) if self.sp % n == 0 and n * n >= self.sp)
        self.nx = self.sp // self.nz
        self.nc = 2
        self.ny = self.tp // self.nc
        self.tok, self.d = shapes["residual"]
        self.own = self.tok // self.tp
        self.heads = shapes["gates"][0]
        self.qk = shapes["queries"][1] // self.heads
        self.vd = shapes["values"][1] // self.heads
        self.per = LANES // self.qk
        self.pairs = self.heads // self.per
        self.vw = shapes["values"][1]
        self.rows, self.ff = shapes["gate"]
        self.zc = self.nz // self.nc
        tiles = self.ff // LANES
        wide = -(-tiles // self.zc)
        starts = [min(i * wide, tiles - wide) for i in range(self.zc)]
        self.start = [s * LANES for s in starts]
        self.dup = [(i * wide - s) * LANES for i, s in enumerate(starts)]
        self.hid = wide * LANES
        self.nj = self.rows // LANES
        self.halves = 2
        self.sph = self.sp // self.halves
        self.cw = self.sph * LANES
        self.ns = self.nj * self.halves
        self.toks = self.nz * self.ny * self.own
        self.state_rows = self.pairs * LANES + -(-(self.pairs + 2 * self.heads) // 8) * 8
        self.wc = next(
            n for n in range(self.hid // LANES * LANES, 0, -LANES) if self.d % n == 0
        )
        self.cc = min(self.cw, self.wc)


def dotf(a, b, dims=(((1,), (0,)), ((), ())), precision=None):
    return lax.dot_general(a, b, dims, preferred_element_type=F32, precision=precision)


def split(a):
    high = a.astype(BF16)
    return high, (a - high.astype(F32)).astype(BF16)


def layer(p, *refs):
    (
        residual, queries, keys, values, out_gate, in_gate, forget, extra, head_gain, out_w,
        ff_gain, gate_w, up_w, down_w,
        out, gate_b, up_b, down_b,
        col, gated, xs, zs, carry, tokens, acc, slab, parts, yb, lb, rb, stream, cr, yr, res,
        s1_send, s1_recv, xf_send, xf_recv, pf_send, pf_recv,
        stx_send, stx_recv, stz_send, stz_recv, at_send, at_recv, ay_send, ay_recv,
        gz_right, gz_left, gz_recv, gy_send, gy_recv,
        ry_send, ry_recv, rr_send, rl_send, rl_recv, rr_recv, local,
    ) = refs
    nz, nx, ny, nc = p.nz, p.nx, p.ny, p.nc
    sp_i, tp_i = lax.axis_index("sp"), lax.axis_index("tp")
    z, x = sp_i // nx, lax.rem(sp_i, nx)
    y, c = tp_i // nc, lax.rem(tp_i, nc)
    other = 1 - c
    duty = c == 1 - z // p.zc

    def dev(z_, x_, y_, c_):
        return (z_ * nx + x_, y_ * nc + c_)

    def mod(a, e, n):
        return lax.rem(a + e, n)

    def remote(src, dst, send, recv, device):
        return pltpu.make_async_remote_copy(
            src_ref=src, dst_ref=dst, send_sem=send, recv_sem=recv,
            device_id=device, device_id_type=MESH,
        )

    barrier = pltpu.get_barrier_semaphore()
    friends = [dev(mod(z, e, nz), x, y, c) for e in range(1, nz)]
    friends += [dev(z, mod(x, e, nx), y, c) for e in range(1, nx)]
    friends += [dev(z, x, mod(y, e, ny), c) for e in range(1, ny)]
    friends += [dev(mod(z, e, nz), x, y, other) for e in range(nz)]
    for friend in friends:
        pl.semaphore_signal(barrier, inc=1, device_id=friend, device_id_type=MESH)
    pl.semaphore_wait(barrier, len(friends))

    mats = ((gate_w, gate_b), (up_w, up_b), (down_w, down_b))

    def jrows(j):
        return pl.ds(pl.multiple_of(j * LANES, LANES), LANES)

    def first_hop(m, j, i):
        src, dst = mats[m]
        return remote(
            src.at[jrows(j), pl.ds(p.start[i], p.hid)],
            dst.at[sp_i, jrows(j), :],
            s1_send.at[m, j, i], s1_recv.at[m, j, z],
            dev(c * p.zc + i, x, y, other),
        )

    def first_recv(m, j, zs_):
        src, dst = mats[m]
        view = dst.at[zs_ * nx + x, jrows(j), :]
        return remote(view, view, s1_send.at[m, j, 0], s1_recv.at[m, j, zs_], dev(z, x, y, other))

    def across(m, j, zs_, e):
        view = mats[m][1].at[zs_ * nx + x, jrows(j), :]
        return remote(
            view, view, xf_send.at[m, j, zs_, e - 1], xf_recv.at[m, j, zs_, e - 1],
            dev(z, mod(x, e, nx), y, c),
        )

    def across_recv(m, j, zs_, e):
        view = mats[m][1].at[zs_ * nx + mod(x, nx - e, nx), jrows(j), :]
        return remote(
            view, view, xf_send.at[m, j, zs_, e - 1], xf_recv.at[m, j, zs_, e - 1],
            dev(z, mod(x, e, nx), y, c),
        )

    def to_peer(m, j, sp_):
        view = mats[m][1].at[sp_, jrows(j), :]
        return remote(view, view, pf_send.at[m, j], pf_recv.at[m, j], dev(z, x, y, other))

    def peer_all(m, j):
        view = mats[m][1].at[:, jrows(j), :]
        return remote(view, view, pf_send.at[m, j], pf_recv.at[m, j], dev(z, x, y, other))

    def send_group(ms, j):
        for i in range(p.zc):

            @pl.when(c * p.zc + i != z)
            def _(i=i):
                for m in ms:
                    first_hop(m, j, i).start()

    def send_own():
        for i in range(p.zc):

            @pl.when(c * p.zc + i == z)
            def _(i=i):
                for m in range(3):
                    for j in range(p.nj):
                        first_hop(m, j, i).start()

    def each_other(fn, least=1, most=None):
        for dist in range(least, most or nz):
            pl.when(z - dist >= 0)(functools.partial(fn, z - dist))
            pl.when(z + dist < nz)(functools.partial(fn, z + dist))

    def each_z(fn):
        fn(z)
        each_other(fn)

    def pass_on(ms, j, zs_):
        for m in ms:
            first_recv(m, j, zs_).wait_recv()
            for e in range(1, nx):
                across(m, j, zs_, e).start()
            to_peer(m, j, zs_ * nx + x).start()

    def relay(ms, j, least=1, most=None):
        @pl.when(duty)
        def _():
            each_other(functools.partial(pass_on, ms, j), least, most)

    def relay_near(ms, j):
        relay(ms, j, 1, 2)

    def relay_far(ms, j):
        relay(ms, j, 2)

    def relay_own(ms):
        @pl.when(duty)
        def _():
            for j in range(p.nj):
                pass_on(ms, j, z)

    def settle(ms, j):
        @pl.when(duty)
        def _():
            def one(zs_):
                for m in ms:
                    for e in range(1, nx):
                        across_recv(m, j, zs_, e).wait_recv()
                        to_peer(m, j, zs_ * nx + mod(x, nx - e, nx)).start()

            each_z(one)

        @pl.when(jnp.logical_not(duty))
        def _():
            for m in ms:
                peer_all(m, j).wait_recv()

    send_group((0,), 0)
    send_own()
    fetch_res = pltpu.make_async_copy(
        residual.at[pl.ds(pl.multiple_of(tp_i * p.own, p.own), p.own), :], res, local.at[2]
    )
    fetch_res.start()

    heads, per, pairs, tok = p.heads, p.per, p.pairs, p.tok
    fg = forget[...]
    lf = jnp.minimum(fg, 0.0) - jnp.log1p(jnp.exp(-jnp.abs(fg))) + extra[...]
    upper = (
        lax.broadcasted_iota(jnp.int32, (tok, tok), 0)
        <= lax.broadcasted_iota(jnp.int32, (tok, tok), 1)
    ).astype(F32)
    pad = jnp.zeros((-heads % 8, tok), F32)
    lf8 = jnp.concatenate([lf, pad], axis=0) if pad.shape[0] else lf
    cum_row = dotf(lf8, upper, precision=lax.Precision.HIGHEST)[:heads]
    ig = in_gate[...]
    pad = jnp.zeros((-2 * heads % 8, tok), F32)
    both = [cum_row, ig] + ([pad] if pad.shape[0] else [])
    col[...] = jnp.concatenate(both, axis=0).T
    bias_row = ig - cum_row
    base = pairs * LANES
    lane = lax.broadcasted_iota(jnp.int32, (1, LANES), 1) // p.qk
    subl = lax.broadcasted_iota(jnp.int32, (LANES, 1), 0) // p.qk

    def head_lanes(ref, h):
        pair = ref[:, h // per * LANES : (h // per + 1) * LANES]
        return jnp.where(lane == h % per, pair, jnp.zeros_like(pair))

    for pr in range(pairs):
        state = jnp.zeros((LANES, LANES), F32)
        norm = jnp.zeros((1, LANES), F32)
        for h in range(pr * per, (pr + 1) * per):
            total = cum_row[h : h + 1, tok - 1 : tok]
            log_w = total - col[:, h : h + 1] + col[:, heads + h : heads + h + 1]
            peak = jnp.max(log_w, axis=0, keepdims=True)
            weight = jnp.exp(log_w - peak)
            k_h = head_lanes(keys, h)
            high, low = split(values[:, h * p.vd : (h + 1) * p.vd].astype(F32) * weight)
            over = (((0,), (0,)), ((), ()))
            state += dotf(k_h, high, over) + dotf(k_h, low, over)
            norm += jnp.sum(k_h.astype(F32) * weight, axis=0, keepdims=True)
            row = base + pairs + h
            xs[x, row : row + 1, :] = jnp.broadcast_to(total, (1, LANES))
            row = base + pairs + heads + h
            xs[x, row : row + 1, :] = jnp.broadcast_to(peak, (1, LANES))
        xs[x, pr * LANES : (pr + 1) * LANES, :] = state
        xs[x, base + pr : base + pr + 1, :] = norm
    spare = p.state_rows - base - pairs - 2 * heads
    if spare:
        xs[x, p.state_rows - spare :, :] = jnp.zeros((spare, LANES), F32)

    def state_x(e):
        return remote(
            xs.at[x], xs.at[x], stx_send.at[e - 1], stx_recv.at[e - 1],
            dev(z, mod(x, e, nx), y, c),
        )

    def state_x_recv(e):
        view = xs.at[mod(x, nx - e, nx)]
        return remote(view, view, stx_send.at[e - 1], stx_recv.at[e - 1], dev(z, mod(x, e, nx), y, c))

    for e in range(1, nx):
        state_x(e).start()

    def join(target, later):
        lo = base + pairs
        tot_e, tot_l = target[lo : lo + heads, :], later[lo : lo + heads, :]
        pk_e = target[lo + heads : lo + 2 * heads, :]
        pk_l = later[lo + heads : lo + 2 * heads, :]
        pk = jnp.maximum(tot_l + pk_e, pk_l)
        w_e, w_l = jnp.exp(tot_l + pk_e - pk), jnp.exp(pk_l - pk)
        for pr in range(pairs):
            hs = [pr * per + i for i in range(per)]
            e_col = jnp.zeros((LANES, LANES), F32)
            l_col = jnp.zeros((LANES, LANES), F32)
            e_row = jnp.zeros((1, LANES), F32)
            l_row = jnp.zeros((1, LANES), F32)
            for i, h in enumerate(hs):
                e_col = jnp.where(subl == i, w_e[h : h + 1, :], e_col)
                l_col = jnp.where(subl == i, w_l[h : h + 1, :], l_col)
                e_row = jnp.where(lane == i, w_e[h : h + 1, :], e_row)
                l_row = jnp.where(lane == i, w_l[h : h + 1, :], l_row)
            blk = slice(pr * LANES, (pr + 1) * LANES)
            target[blk, :] = e_col * target[blk, :] + l_col * later[blk, :]
            row = slice(base + pr, base + pr + 1)
            target[row, :] = e_row * target[row, :] + l_row * later[row, :]
        target[lo : lo + heads, :] = tot_e + tot_l
        target[lo + heads : lo + 2 * heads, :] = pk

    def reset(target):
        target[...] = jnp.zeros((p.state_rows, LANES), F32)
        lo = base + pairs + heads
        target[lo : lo + heads, :] = jnp.full((heads, LANES), -1e30, F32)

    for e in range(1, nx):
        state_x_recv(e).wait_recv()
    mine = zs.at[z]
    reset(mine)
    for i in range(nx):
        join(mine, xs.at[i])

    def state_z(dist):
        return remote(
            zs.at[z], zs.at[z], stz_send.at[dist - 1], stz_recv.at[z],
            dev(lax.rem(z + dist, nz), x, y, c),
        )

    for dist in range(1, nz):
        pl.when(z + dist < nz)(lambda dist=dist: state_z(dist).start())
    send_group((1,), 0)
    for j in range(1, min(EARLY_GROUPS, p.nj)):
        send_group((0, 1), j)
    relay_own((0, 1))

    reset(carry)
    for i in range(nz - 1):

        @pl.when(i < z)
        def _(i=i):
            remote(zs.at[i], zs.at[i], stz_send.at[0], stz_recv.at[i], dev(z, x, y, other)).wait_recv()
            join(carry, zs.at[i])

    for i in range(nx - 1):
        pl.when(i < x)(lambda i=i: join(carry, xs.at[i]))

    lo = base + pairs
    total_in = carry[lo : lo + heads, :]
    peak_raw = carry[lo + heads : lo + 2 * heads, :]
    peak_all = jnp.maximum(peak_raw, total_in)
    scale_all = jnp.exp(peak_raw - peak_all)
    unit = p.qk ** (-0.5)
    qrows = min(QUERY_ROWS, tok)
    for h in range(heads):
        pr = h // per
        peak_in = peak_all[h : h + 1, 0:1]
        scale = scale_all[h : h + 1, :]
        st_high, st_low = split(carry[pr * LANES : (pr + 1) * LANES, :] * scale)
        norm_in = carry[base + pr : base + pr + 1, :] * scale
        k2 = keys[:, pr * LANES : (pr + 1) * LANES]
        v_h = values[:, h * p.vd : (h + 1) * p.vd]
        for r0 in range(0, tok, qrows):
            r1 = r0 + qrows
            q2 = queries[r0:r1, pr * LANES : (pr + 1) * LANES]
            q_h = jnp.where(lane == h % per, q2, jnp.zeros_like(q2))
            cum_c = col[r0:r1, h : h + 1]
            seen = (
                lax.broadcasted_iota(jnp.int32, (qrows, r1), 0) + r0
                >= lax.broadcasted_iota(jnp.int32, (qrows, r1), 1)
            )
            logs = jnp.where(seen, bias_row[h : h + 1, :r1], -jnp.inf) + cum_c
            inter = cum_c + peak_in
            peak_row = jnp.maximum(inter, jnp.max(logs, axis=1, keepdims=True))
            dots = dotf(q_h, k2[:r1], (((1,), (1,)), ((), ()))) * unit
            probs = dots * jnp.exp(logs - peak_row)
            inter_scale = jnp.exp(inter - peak_row) * unit
            high, low = split(probs)
            numer = dotf(high, v_h[:r1]) + dotf(low, v_h[:r1])
            numer += inter_scale * (dotf(q_h, st_high) + dotf(q_h, st_low))
            denom = jnp.sum(probs, axis=1, keepdims=True) + inter_scale * jnp.sum(
                q_h.astype(F32) * norm_in, axis=1, keepdims=True
            )
            cell = numer / jnp.maximum(jnp.abs(denom), jnp.exp(-peak_row))
            square = jnp.mean(cell * cell, axis=1, keepdims=True)
            span = slice(h * p.vd, (h + 1) * p.vd)
            gain = head_gain[:, span].astype(F32)
            gates = jax.nn.sigmoid(out_gate[r0:r1, span].astype(F32))
            gated[r0:r1, span] = (cell * lax.rsqrt(square + 1e-06) * gain * gates).astype(BF16)

    pieces = p.d // p.wc

    def fetch_w(n):
        return pltpu.make_async_copy(
            out_w.at[:, pl.ds(n * p.wc, p.wc)],
            slab.at[n % 2, pl.ds(0, p.vw), pl.ds(0, p.wc)],
            local.at[n % 2],
        )

    fetch_w(0).start()
    for n in range(pieces):
        if n + 1 < pieces:
            fetch_w(n + 1).start()
        fetch_w(n).wait()
        for c0 in range(0, p.wc, p.cc):
            g0 = n * p.wc + c0
            w = slab[n % 2, : p.vw, c0 : c0 + p.cc]
            res_ = dotf(gated[...], w).astype(BF16)
            for b in range(p.tp):
                parts[g0 // p.cw, b // ny, b % ny, :, g0 % p.cw : g0 % p.cw + p.cc] = res_[
                    b * p.own : (b + 1) * p.own
                ]

    cols_used = p.d // p.cw

    def at_peer(yy):
        b = yy * nc + other
        return remote(
            parts.at[pl.ds(0, cols_used), b // ny, lax.rem(b, ny)],
            cr.at[:, yy], at_send.at[yy], at_recv.at[yy], dev(z, x, y, other),
        )

    for yy in range(ny):
        at_peer(yy).start()

    def at_y(e):
        b = mod(y, e, ny) * nc + c
        return remote(
            parts.at[pl.ds(0, cols_used), b // ny, lax.rem(b, ny)],
            yr.at[:, e - 1], ay_send.at[e - 1], ay_recv.at[e - 1], dev(z, x, mod(y, e, ny), c),
        )

    for yy in range(ny):
        at_peer(yy).wait_recv()
    for e in range(1, ny):
        to = mod(y, e, ny)
        b = to * nc + c
        for n in range(cols_used):
            parts[n, b // ny, lax.rem(b, ny)] = (
                parts[n, b // ny, lax.rem(b, ny)].astype(F32) + cr[n, to].astype(F32)
            ).astype(BF16)
        at_y(e).start()
    fetch_res.wait()
    b = y * nc + c
    for n in range(cols_used):
        cols = slice(n * p.cw, (n + 1) * p.cw)
        stream[:, cols] = (
            res[:, cols].astype(F32)
            + parts[n, b // ny, lax.rem(b, ny)].astype(F32) + cr[n, y].astype(F32)
        )
    relay((0, 1), 0)
    for e in range(1, ny):
        at_y(e).wait_recv()
        for n in range(cols_used):
            cols = slice(n * p.cw, (n + 1) * p.cw)
            stream[:, cols] += yr[n, e - 1].astype(F32)
    cut = p.own // GATHER_CUTS
    for s in range(GATHER_CUTS):
        rows = slice(s * cut, (s + 1) * cut)
        part = stream[rows, :]
        square = jnp.mean(part * part, axis=1, keepdims=True)
        tokens[z, y, rows, :] = (
            part * lax.rsqrt(square + 1e-06) * ff_gain[...].astype(F32)
        ).astype(BF16)

    def block(zz, yy, s):
        return tokens.at[zz, yy, pl.ds(s * cut, cut), :]

    def go_right(zz, s):
        return remote(block(zz, y, s), block(zz, y, s), gz_right.at[zz, s], gz_recv.at[zz, s],
                      dev(z + 1, x, y, c))

    def go_left(zz, s):
        return remote(block(zz, y, s), block(zz, y, s), gz_left.at[zz, s], gz_recv.at[zz, s],
                      dev(z - 1, x, y, c))

    def go_y(zz, s, e):
        return remote(block(zz, y, s), block(zz, y, s), gy_send.at[zz, s, e - 1],
                      gy_recv.at[zz, s, e - 1], dev(z, x, mod(y, e, ny), c))

    def y_recv(zz, s, e):
        view = block(zz, mod(y, ny - e, ny), s)
        return remote(view, view, gy_send.at[zz, s, e - 1], gy_recv.at[zz, s, e - 1],
                      dev(z, x, mod(y, e, ny), c))

    for s in range(GATHER_CUTS):
        pl.when(z + 1 < nz)(lambda s=s: go_right(z, s).start())
        pl.when(z >= 1)(lambda s=s: go_left(z, s).start())
        for e in range(1, ny):
            go_y(z, s, e).start()
    relay_own((2,))
    for j in range(1, min(EARLY_GROUPS, p.nj)):
        relay((0, 1), j)
    for dist in range(1, nz):
        for s in range(GATHER_CUTS):

            @pl.when(z - dist >= 0)
            def _(dist=dist, s=s):
                go_right(z - dist, s).wait_recv()
                pl.when(z + 1 < nz)(lambda: go_right(z - dist, s).start())
                for e in range(1, ny):
                    go_y(z - dist, s, e).start()

            @pl.when(z + dist < nz)
            def _(dist=dist, s=s):
                go_left(z + dist, s).wait_recv()
                pl.when(z >= 1)(lambda: go_left(z + dist, s).start())
                for e in range(1, ny):
                    go_y(z + dist, s, e).start()

    for j in range(min(EARLY_GROUPS, p.nj), p.nj):
        send_group((0, 1), j)
    for j in range(p.nj):
        send_group((2,), j)
    for j in range(min(EARLY_GROUPS, p.nj)):
        settle((0, 1), j)
    if p.nj > EARLY_GROUPS:
        relay((0, 1), EARLY_GROUPS)
    for zz in range(nz):
        for s in range(GATHER_CUTS):
            for e in range(1, ny):
                y_recv(zz, s, e).wait_recv()
    for s in range(GATHER_CUTS):

        def sent(zz, s=s):
            pl.when((z + 1 < nz) & (zz <= z))(lambda: go_right(zz, s).wait_send())
            pl.when((z >= 1) & (zz >= z))(lambda: go_left(zz, s).wait_send())
            for e in range(1, ny):
                go_y(zz, s, e).wait_send()

        for zz in range(nz):
            sent(zz)

    trows = p.ny * p.own

    def load_slab(m, j):
        return [
            pltpu.make_async_copy(
                mats[m][1].at[s, jrows(j), :],
                slab.at[m, pl.ds(s * LANES, LANES), :],
                local.at[m],
            )
            for s in range(p.sp)
        ]

    def whole_slab(m):
        return pltpu.make_async_copy(slab.at[m], slab.at[m], local.at[m])

    for j in range(p.nj):
        if j >= EARLY_GROUPS:
            coming = ((0, 1), j + 1) if j + 1 < p.nj else ((2,), 0)
            relay_near(*coming)
            settle((0, 1), j)
            if j + 1 < p.nj:
                relay_far(*coming)
        for m in range(2):
            for copy in load_slab(m, j):
                copy.start()
        for m in range(2):
            whole_slab(m).wait()

        @pl.loop(0, nz)
        def _(zz, j=j):
            lhs = jnp.concatenate(
                [
                    tokens[zz, :, :, s * p.rows + j * LANES : s * p.rows + (j + 1) * LANES].reshape(
                        trows, LANES
                    )
                    for s in range(p.sp)
                ],
                axis=1,
            )
            for m in range(2):
                more = dotf(lhs, slab[m])
                if j == 0:
                    acc[zz, m] = more
                else:
                    acc[zz, m] += more

    if p.nj <= EARLY_GROUPS:
        relay((2,), 0)
    else:
        relay_far((2,), 0)
    if p.nj > 1:
        relay((2,), 1)

    @pl.loop(0, nz)
    def _(zz):
        hidden = jax.nn.silu(acc[zz, 0]) * acc[zz, 1]
        if any(p.dup):
            seen_col = lax.broadcasted_iota(jnp.int32, (1, p.hid), 1)
            for i in range(p.zc):
                if p.dup[i]:
                    drop = (seen_col < p.dup[i]) & (lax.rem(z, p.zc) == i)
                    hidden = jnp.where(drop, 0.0, hidden)
        tokens[zz, :, :, : p.hid] = hidden.astype(BF16).reshape(ny, p.own, p.hid)

    def ry(n, e):
        return remote(
            parts.at[n, :, mod(y, e, ny)], yb.at[n, e - 1], ry_send.at[n, e - 1],
            ry_recv.at[n, e - 1], dev(z, x, mod(y, e, ny), c),
        )

    def rz_right(n, o):
        return remote(parts.at[n, o, y], lb.at[n, o - 1], rr_send.at[n, o], rl_recv.at[n, o],
                      dev(z + 1, x, y, c))

    def rz_left(n, o):
        return remote(parts.at[n, o, y], rb.at[n, o], rl_send.at[n, o], rr_recv.at[n, o],
                      dev(z - 1, x, y, c))

    for yy in range(ny):
        at_peer(yy).wait_send()
    for e in range(1, ny):
        at_y(e).wait_send()

    def add_stream(n, more):
        j, half = n // p.halves, lax.rem(n, p.halves)
        for q in range(p.sph):
            at = pl.multiple_of((half * p.sph + q) * p.rows + j * LANES, LANES)
            stream[:, pl.ds(at, LANES)] += 0.5 * more[:, q * LANES : (q + 1) * LANES]

    def load_down(n):
        j, half = n // p.halves, lax.rem(n, p.halves)
        return [
            pltpu.make_async_copy(
                down_b.at[half * p.sph + q, jrows(j), :],
                slab.at[0, pl.ds(q * LANES, LANES), :],
                local.at[0],
            )
            for q in range(p.sph)
        ]

    def step(i, _):
        @pl.when(i < p.ns)
        def _():
            j = i // p.halves

            @pl.when(lax.rem(i, p.halves) == 0)
            def _():
                settle((2,), j)

            for copy in load_down(i):
                copy.start()
            view = slab.at[0, pl.ds(0, p.sph * LANES), :]
            pltpu.make_async_copy(view, view, local.at[0]).wait()

            @pl.loop(0, nz)
            def _(zz):
                hid = tokens[zz, :, :, : p.hid].reshape(trows, p.hid)
                terms = dotf(hid, slab[0, : p.sph * LANES, :], (((1,), (1,)), ((), ())))
                parts[i, zz] = terms.astype(BF16).reshape(ny, p.own, p.cw)

            for e in range(1, ny):
                ry(i, e).start()

            @pl.when((lax.rem(i, p.halves) == 0) & (j + 2 < p.nj))
            def _():
                relay((2,), j + 2)

        @pl.when((i >= 1) & (i <= p.ns))
        def _():
            n = i - 1
            for e in range(1, ny):
                ry(n, e).wait_recv()

            @pl.loop(0, nz)
            def _(o):
                total = parts[n, o, y].astype(F32)
                for e in range(1, ny):
                    total += yb[n, e - 1, o].astype(F32)
                parts[n, o, y] = total.astype(BF16)
                pl.when(o == z)(lambda: add_stream(n, total))

        right = i - 1 - z

        @pl.when((right >= 0) & (right < p.ns))
        def _():
            for o in range(nz - 1, 0, -1):

                @pl.when((o >= z) & (z > 0))
                def _(o=o):
                    rz_right(right, o).wait_recv()

                @pl.when((o > z) & (z > 0))
                def _(o=o):
                    parts[right, o, y] = (
                        parts[right, o, y].astype(F32) + lb[right, o - 1].astype(F32)
                    ).astype(BF16)

                pl.when(o > z)(lambda o=o: rz_right(right, o).start())
                pl.when(o == z)(lambda o=o: add_stream(right, lb[right, o - 1].astype(F32)))

        left = i - 1 - (nz - 1 - z)

        @pl.when((left >= 0) & (left < p.ns))
        def _():
            for o in range(nz - 1):

                @pl.when((o <= z) & (z < nz - 1))
                def _(o=o):
                    rz_left(left, o).wait_recv()

                @pl.when((o < z) & (z < nz - 1))
                def _(o=o):
                    parts[left, o, y] = (
                        parts[left, o, y].astype(F32) + rb[left, o].astype(F32)
                    ).astype(BF16)

                pl.when(o < z)(lambda o=o: rz_left(left, o).start())
                pl.when(o == z)(lambda o=o: add_stream(left, rb[left, o].astype(F32)))

        return 0

    lax.fori_loop(0, p.ns + nz, step, 0)
    out[...] = stream[...].astype(BF16)

    for e in range(1, nx):
        state_x(e).wait_send()
    for dist in range(1, nz):
        pl.when(z + dist < nz)(lambda dist=dist: state_z(dist).wait_send())

    @pl.loop(0, p.nj)
    def _(j):
        for m in range(3):
            for i in range(p.zc):
                first_hop(m, j, i).wait_send()

            @pl.when(duty)
            def _(m=m):
                for zz in range(nz):
                    for e in range(1, nx):
                        across(m, j, zz, e).wait_send()
                peer_all(m, j).wait_send()

    @pl.loop(0, p.ns)
    def _(n):
        for e in range(1, ny):
            ry(n, e).wait_send()
        for o in range(nz):
            if o:
                pl.when(o > z)(lambda o=o: rz_right(n, o).wait_send())
            if o < nz - 1:
                pl.when(o < z)(lambda o=o: rz_left(n, o).wait_send())


def solution(mesh):
    def per_device(*args):
        (residual, queries, keys, values, out_gate, in_gate, forget, extra, head_gain, out_w,
         ff_gain, gate_w, up_w, down_w) = args
        p = Plan(
            dict(mesh.shape),
            {
                "residual": residual.shape, "queries": queries.shape, "values": values.shape,
                "gates": in_gate.shape, "gate": gate_w.shape,
            },
        )
        vmem = pl.BlockSpec(memory_space=pltpu.VMEM)
        hbm = pl.BlockSpec(memory_space=pl.ANY)
        dma = pltpu.SemaphoreType.DMA
        held = jax.ShapeDtypeStruct((p.sp, p.rows, p.hid), BF16)
        nj, nz, nx, ny, ns = p.nj, p.nz, p.nx, p.ny, p.ns
        cols_used = p.d // p.cw
        cols8 = -(-2 * p.heads // 8) * 8
        scratch = [
            pltpu.VMEM((p.tok, cols8), F32),
            pltpu.VMEM((p.tok, p.vw), BF16),
            pltpu.VMEM((nx, p.state_rows, LANES), F32),
            pltpu.VMEM((nz, p.state_rows, LANES), F32),
            pltpu.VMEM((p.state_rows, LANES), F32),
            pltpu.VMEM((nz, ny, p.own, p.d), BF16),
            pltpu.VMEM((nz, 2, ny * p.own, p.hid), F32),
            pltpu.VMEM((2, p.sp * LANES, p.hid), BF16),
            pltpu.VMEM((ns, nz, ny, p.own, p.cw), BF16),
            pltpu.VMEM((ns, ny - 1, nz, p.own, p.cw), BF16),
            pltpu.VMEM((ns, nz - 1, p.own, p.cw), BF16),
            pltpu.VMEM((ns, nz - 1, p.own, p.cw), BF16),
            pltpu.VMEM((p.own, p.d), F32),
            pltpu.VMEM((cols_used, ny, p.own, p.cw), BF16),
            pltpu.VMEM((cols_used, ny - 1, p.own, p.cw), BF16),
            pltpu.VMEM((p.own, p.d), BF16),
            dma((3, nj, p.zc)), dma((3, nj, nz)),
            dma((3, nj, nz, nx - 1)), dma((3, nj, nz, nx - 1)),
            dma((3, nj)), dma((3, nj)),
            dma((nx - 1,)), dma((nx - 1,)),
            dma((nz - 1,)), dma((nz,)),
            dma((ny,)), dma((ny,)), dma((ny - 1,)), dma((ny - 1,)),
            dma((nz, GATHER_CUTS)), dma((nz, GATHER_CUTS)), dma((nz, GATHER_CUTS)),
            dma((nz, GATHER_CUTS, ny - 1)), dma((nz, GATHER_CUTS, ny - 1)),
            dma((ns, ny - 1)), dma((ns, ny - 1)),
            dma((ns, nz)), dma((ns, nz)), dma((ns, nz)), dma((ns, nz)),
            dma((3,)),
        ]
        result = pl.pallas_call(
            functools.partial(layer, p),
            out_shape=(
                jax.ShapeDtypeStruct((p.own, p.d), BF16), held, held, held,
            ),
            in_specs=[hbm] + [vmem] * 8 + [hbm, vmem] + [hbm] * 3,
            out_specs=(vmem, hbm, hbm, hbm),
            scratch_shapes=scratch,
            compiler_params=pltpu.CompilerParams(
                collective_id=0, has_side_effects=True, vmem_limit_bytes=67043328
            ),
            name="layer",
        )(
            residual, queries, keys, values, out_gate, in_gate, forget, extra,
            head_gain.reshape(1, -1), out_w, ff_gain.reshape(1, -1), gate_w, up_w, down_w,
        )
        return result[0]

    in_specs = (
        P("sp", None), P("sp", "tp"), P("sp", "tp"), P("sp", "tp"), P("sp", "tp"),
        P("tp", "sp"), P("tp", "sp"), P("tp", "sp"), P("tp"), P("tp", None), P(),
        P("sp", "tp"), P("sp", "tp"), P("sp", "tp"),
    )
    return jax.shard_map(
        per_device, mesh=mesh, in_specs=in_specs, out_specs=P(("sp", "tp"), None), check_vma=False
    )
```
